1024 devices in a mesh: ep: 64 (over z, y), tp: 16 (over x, core).
Axes of the slice: x: 8, y: 8, z: 8, core: 2. Of those that a mesh axis runs over, the one named last changes fastest.
Arguments:
- tokens: bfloat16 [512, 2048], P('ep'), may hold values from -48 to 48
- past_lengths: int32 [512], P('ep'), may hold values from 1024 to 16383
- state: float32 [512, 16, 128, 256], P('ep', 'tp'), may hold values from -0.625 to 0.625
- norm1_gain: float32 [2048], replicated, may hold values from 0.1 to 1.9
- query_weight: bfloat16 [2048, 2048], P(None, 'tp'), may hold values from -0.125 to 0.125
- key_weight: bfloat16 [2048, 2048], P(None, 'tp'), may hold values from -0.125 to 0.125
- value_weight: bfloat16 [2048, 4096], P(None, 'tp'), may hold values from -0.125 to 0.125
- out_weight: bfloat16 [4096, 2048], P('tp'), may hold values from -0.09375 to 0.09375
- norm2_gain: float32 [2048], replicated, may hold values from 0.1 to 1.9
- branch_gate: float32 [2048], replicated, may hold values from -0.125 to 0.125
- route_ids: int32 [512, 2], P('ep'), may hold values from 0 to 15, all different within a row; in each aligned block of 8 rows (0 to 7, 8 to 15, ...) at most 2 rows name the same one
- route_weights: float32 [512, 2], P('ep'), may hold values from 0.2 to 1
- expert_gate: bfloat16 [64, 2048, 1792], P('ep', None, 'tp'), may hold values from -0.125 to 0.125
- expert_up: bfloat16 [64, 2048, 1792], P('ep', None, 'tp'), may hold values from -0.125 to 0.125
- expert_down: bfloat16 [64, 1792, 2048], P('ep', 'tp'), may hold values from -0.0625 to 0.0625
- dense_gate: bfloat16 [2048, 5632], P('tp', 'ep'), may hold values from -0.125 to 0.125
- dense_up: bfloat16 [2048, 5632], P('tp', 'ep'), may hold values from -0.125 to 0.125
- dense_down: bfloat16 [5632, 2048], P('ep', 'tp'), may hold values from -0.15625 to 0.15625
Outputs:
- layer_out: bfloat16 [512, 2048], P('ep', 'tp')
- new_state: float32 [512, 16, 128, 256], P('ep', 'tp')
The draws below stay inside these ranges and needn't reach their ends.
Inputs may be any that keep to these rules, and one draw needn't show every extreme that they name: `route_ids`: in each aligned block of 8 rows no expert is named by more than 2 rows, and some block names one expert exactly 2 times.
All inputs are finite; a program needn't handle non-finite values.
Results may differ from the reference program's by a relative error of at most 0.006.
Values may be sent and summed in bfloat16 or wider, within the bound.
No kernel may reach another device: no remote copies, remote signals or barrier semaphores. Data moves between devices by JAX's collectives and lax.ppermute only.
A program may use at most 64 MiB of HBM per device.

```python
import math
import jax
import jax.numpy as jnp
import numpy as np
from jax import lax

G = 8
TOKENS = 512
D = 2048
H = 16
DK = 128
DV = 256
FF = 5632
EXP_FF = 7168
TOPK = 2
EXPERTS = 16
CAP = 2


def draw_tokens(key, part):
    first_key, second_key = jax.random.split(jax.random.fold_in(key, 11), 2)
    columns = jnp.arange(D, dtype=jnp.float32) / D
    base = jax.random.truncated_normal(first_key, -4.0, 4.0, (TOKENS, D), jnp.float32)
    col_scale = jnp.exp(jnp.log(3.0) * columns)
    row_scale = jnp.exp(jax.random.uniform(second_key, (TOKENS, 1), jnp.float32, jnp.log(0.5), jnp.log(3.0)))
    return (base * col_scale[None, :] * row_scale).astype(jnp.bfloat16)


def touch_ends(result, rng, low, top_value):
    longest = result.shape.index(max(result.shape))
    spots = []
    for shift in (0, 1):
        where = [jax.random.randint(jax.random.fold_in(rng, axis), (), 0, length) for axis, length in enumerate(result.shape)]
        where[longest] = (where[longest] + shift) % result.shape[longest]
        spots.append(tuple(where))
    return result.at[spots[0]].set(low).at[spots[1]].set(top_value)


def shard_levels(rng, shape, cuts, smallest, high):
    def one(position, parts):
        steps = jax.random.uniform(jax.random.fold_in(jax.random.fold_in(rng, 6), position), (parts,), jnp.float32, smallest / len(cuts), high / len(cuts))
        return jnp.repeat(jnp.exp(steps), shape[position] // parts).reshape((-1,) + (1,) * (len(shape) - position - 1))

    factor_of = one(*cuts[0])
    for cut in cuts[1:]:
        factor_of = factor_of * one(*cut)
    return factor_of


def assign_block(stream_key, own, number, rows, amount, top, limit, lean):
    order = jax.random.permutation(stream_key, amount)
    packed, ordinary = shares(amount, rows * top, limit, lean, True), shares(amount, rows * top, limit, lean, False)
    places = jnp.arange(amount)

    def named(lengths, turn):
        used = int((lengths > 0).sum())
        fixed = max(1, used // 4)
        moved = fixed + (places - fixed + turn * (used - fixed)) % max(1, amount - fixed)
        return jnp.zeros((amount,), jnp.int32).at[order[jnp.where(places < fixed, places, moved)]].set(jnp.asarray(lengths, jnp.int32))

    lengths = jnp.where(number % 4 == 0, named(packed, number // 4), named(ordinary, number - number // 4 - 1))
    mixed = jax.random.permutation(jax.random.fold_in(own, 3), amount)
    source_of, sink = mixed[0:amount // 2 * 2:2], mixed[1:amount // 2 * 2:2]
    slack = jnp.minimum(lengths[source_of] - 1, limit - lengths[sink]) // 2
    slack = jnp.where((source_of == order[0]) | (sink == order[0]) | (lengths[sink] == 0), 0, jnp.maximum(slack, 0))
    moved = jax.random.randint(jax.random.fold_in(own, 4), (amount // 2,), 0, 1 << 20) % (slack + 1)
    lengths = lengths.at[source_of].add(-moved).at[sink].add(moved)
    members = jnp.searchsorted(jnp.cumsum(lengths), jnp.arange(rows * top), side="right").astype(jnp.int32)
    table = members.reshape(top, rows).T
    table = table[jax.random.permutation(jax.random.fold_in(own, 1), rows)]
    turn = jax.random.randint(jax.random.fold_in(own, 2), (rows, 1), 0, top)
    return jnp.take_along_axis(table, (jnp.arange(top)[None, :] + turn) % top, axis=1)


def shares(count, total, bound, lean, full):
    portions = [(1 << 20) // math.isqrt(rank ** lean) + 1 for rank in range(1, count + 1)]
    largest = bound if full else min(bound, max(-(-total // count), total * portions[0] // sum(portions)))
    least = 1 if total - largest >= count - 1 else 0
    given, spare = [largest] + [least] * (count - 1), total - largest - least * (count - 1)
    while spare > 0:
        free = [i for i in range(1, count) if given[i] < largest] or [i for i in range(1, count) if given[i] < bound]
        pool, left = sum([portions[i] for i in free]), spare
        for i in free:
            extra = min(bound - given[i], max(1, left * portions[i] // pool), spare)
            given[i] = given[i] + extra
            spare = spare - extra
    return np.array(given)


def normal_values(stream_key, shape, deviation, most, cuts=(), kind=jnp.bfloat16):
    drawn = jax.random.normal(stream_key, shape, jnp.float32) * deviation
    if len(cuts) > 0:
        drawn = shard_levels(stream_key, shape, cuts, -0.22, 0.18) * drawn
    return jnp.clip(drawn, min=-most, max=most).astype(kind)


def setup_inputs(seed: int = 0) -> dict:
    streams_of = jax.random.split(jax.random.key(seed), 19)
    tokens = draw_tokens(jax.random.fold_in(streams_of[18], 71), 0)
    past_lengths = touch_ends(jax.random.randint(streams_of[1], (TOKENS,), 1024, 16384), jax.random.fold_in(streams_of[1], 1), 1024, 16383).astype(jnp.int32)
    state = normal_values(streams_of[2], (TOKENS, H, DK, DV), 0.1, 0.625, ((0, 64), (1, 16)), jnp.float32)
    norm1_gain = jnp.clip(1.0 + 0.18 * jax.random.normal(streams_of[3], (D,), jnp.float32), 0.1, 1.9)
    query_weight = normal_values(streams_of[4], (D, H * DK), D ** -0.5, 0.125, ((1, 16),))
    key_weight = normal_values(streams_of[5], (D, H * DK), D ** -0.5, 0.125, ((1, 16),))
    value_weight = normal_values(streams_of[6], (D, H * DV), D ** -0.5, 0.125, ((1, 16),))
    out_weight = normal_values(streams_of[7], (H * DV, D), (H * DV) ** -0.5, 0.09375, ((0, 16),))
    norm2_gain = jnp.clip(1.0 + 0.18 * jax.random.normal(streams_of[8], (D,), jnp.float32), 0.1, 1.9)
    branch_gate = normal_values(streams_of[9], (D,), D ** -0.5, 0.125, (), jnp.float32)
    route_ids_keys = jax.random.split(jax.random.fold_in(streams_of[10], 1), TOKENS // G)
    route_ids_turns = jax.random.permutation(jax.random.fold_in(streams_of[10], 3), TOKENS // G)
    route_ids = jax.vmap(lambda own, number: assign_block(jax.random.fold_in(streams_of[10], 2), own, number, G, EXPERTS, TOPK, CAP, 1))(route_ids_keys, route_ids_turns).reshape((TOKENS, TOPK))
    route_weights = jnp.clip(0.2 + 0.8 * jax.random.uniform(streams_of[11], (TOKENS, TOPK), jnp.float32) ** shard_levels(streams_of[11], (TOKENS, TOPK), ((0, 64),), -0.2, 0.2), 0.2, 1.0)
    expert_gate = normal_values(streams_of[12], (4 * EXPERTS, D, EXP_FF // 4), D ** -0.5, 0.125, ((0, 64), (2, 16)))
    expert_up = normal_values(streams_of[13], (4 * EXPERTS, D, EXP_FF // 4), D ** -0.5, 0.125, ((0, 64), (2, 16)))
    expert_down = normal_values(streams_of[14], (4 * EXPERTS, EXP_FF // 4, D), EXP_FF ** -0.5, 0.0625, ((0, 64), (1, 16)))
    dense_gate = normal_values(streams_of[15], (D, FF), D ** -0.5, 0.125, ((0, 16), (1, 64)))
    dense_up = normal_values(streams_of[16], (D, FF), D ** -0.5, 0.125, ((0, 16), (1, 64)))
    dense_down = normal_values(streams_of[17], (FF, D), (FF // 4) ** -0.5, 0.15625, ((0, 64), (1, 16)))
    return {"tokens": tokens, "past_lengths": past_lengths, "state": state, "norm1_gain": norm1_gain, "query_weight": query_weight, "key_weight": key_weight, "value_weight": value_weight, "out_weight": out_weight, "norm2_gain": norm2_gain, "branch_gate": branch_gate, "route_ids": route_ids, "route_weights": route_weights, "expert_gate": expert_gate, "expert_up": expert_up, "expert_down": expert_down, "dense_gate": dense_gate, "dense_up": dense_up, "dense_down": dense_down}


RMS_EPSILON = 1e-06
GROUP_EPSILON = 1e-05
PRECISE = lax.Precision.HIGHEST

def head_decay(head_index, head_total):
    return jnp.exp(jnp.log1p(-jnp.exp2(-5.0 - 7.0 * head_index.astype(jnp.float32) / (head_total - 1))))

def rotate_heads(features, positions):
    half_size = features.shape[-1] // 2
    inverse = 10000.0 ** (-jnp.arange(half_size, dtype=jnp.float32) / half_size)
    angles = positions.astype(jnp.float32)[:, None] * inverse[None, :]
    cosine = jnp.cos(angles)[:, None, :]
    sine_part = jnp.sin(angles)[:, None, :]
    first_half = features[..., :half_size]
    second_half = features[..., half_size:]
    return jnp.concatenate([first_half * cosine - second_half * sine_part, first_half * sine_part + second_half * cosine], axis=-1)

def retention_step(normed_in, positions, state, query_weight, key_weight, value_weight, head_index, head_total):
    row_count, head_count, key_size, value_size = state.shape
    query = jnp.dot(normed_in, query_weight, preferred_element_type=jnp.float32).reshape(row_count, head_count, key_size)
    keys = jnp.dot(normed_in, key_weight, preferred_element_type=jnp.float32).reshape(row_count, head_count, key_size)
    values = jnp.dot(normed_in, value_weight, preferred_element_type=jnp.float32).reshape(row_count, head_count, value_size)
    query = rotate_heads(query, positions)
    keys = rotate_heads(keys, positions) * key_size ** (-0.5)
    decay = head_decay(head_index, head_total)
    new_state = state * decay[None, :, None, None] + keys[:, :, :, None] * values[:, :, None, :]
    retained = jnp.einsum('shk,shkv->shv', query, new_state, precision=PRECISE)
    centered = retained - lax.optimization_barrier(jnp.mean(retained, axis=-1, keepdims=True))
    normed = centered * lax.rsqrt(lax.optimization_barrier(jnp.mean(centered * centered, axis=-1, keepdims=True)) + GROUP_EPSILON)
    return (normed.astype(jnp.bfloat16).reshape(row_count, head_count * value_size), new_state)

def reference(tokens, past_lengths, state, norm1_gain, query_weight, key_weight, value_weight, out_weight, norm2_gain, branch_gate, route_ids, route_weights, expert_gate, expert_up, expert_down, dense_gate, dense_up, dense_down):
    inputs = tokens.astype(jnp.float32)
    normed_in = (inputs * lax.rsqrt(lax.optimization_barrier(jnp.mean(inputs * inputs, axis=-1, keepdims=True)) + RMS_EPSILON) * norm1_gain).astype(jnp.bfloat16)
    head_total = state.shape[1]
    normed, new_state = retention_step(normed_in, past_lengths, state, query_weight, key_weight, value_weight, jnp.arange(head_total), head_total)
    mixed = inputs + jnp.dot(normed, out_weight, preferred_element_type=jnp.float32)
    scale = lax.rsqrt(lax.optimization_barrier(jnp.mean(mixed * mixed, axis=-1, keepdims=True)) + RMS_EPSILON)
    scaled = mixed * scale * norm2_gain
    branch_weight = jax.nn.sigmoid(lax.optimization_barrier(jnp.sum(scaled * branch_gate, axis=-1, keepdims=True)))
    normed_out = scaled.astype(jnp.bfloat16)
    model_width = tokens.shape[1]
    group_count = tokens.shape[0] // G
    route_flat = route_ids.reshape(group_count, G * TOPK)
    onehot = (route_flat[:, :, None] == jnp.arange(EXPERTS, dtype=jnp.int32)[None, None, :]).astype(jnp.int32)
    earlier = jnp.cumsum(onehot, axis=1) - onehot
    slot_index = lax.optimization_barrier(jnp.sum(earlier * onehot, axis=2))
    target = route_flat * CAP + slot_index
    placed = (target[:, :, None] == jnp.arange(EXPERTS * CAP, dtype=jnp.int32)[None, None, :]).astype(jnp.float32)
    placed = placed.reshape(group_count, G, TOPK, EXPERTS * CAP)
    selector = lax.optimization_barrier(jnp.sum(placed, axis=2))
    combiner = lax.optimization_barrier(jnp.sum(placed * route_weights.reshape(group_count, G, TOPK, 1), axis=2))
    grouped = normed_out.reshape(group_count, G, model_width).astype(jnp.float32)
    buffers = jnp.einsum('gtp,gtd->gpd', selector, grouped, precision=PRECISE).astype(jnp.bfloat16)
    expert_rows = buffers.reshape(group_count, EXPERTS, CAP, model_width).transpose(1, 0, 2, 3).reshape(EXPERTS, group_count * CAP, model_width)
    quarter = expert_gate.shape[2]
    gate_full = expert_gate.reshape(EXPERTS, 4, model_width, quarter).transpose(0, 2, 1, 3).reshape(EXPERTS, model_width, 4 * quarter)
    up_full = expert_up.reshape(EXPERTS, 4, model_width, quarter).transpose(0, 2, 1, 3).reshape(EXPERTS, model_width, 4 * quarter)
    down_full = expert_down.reshape(EXPERTS, 4 * quarter, model_width)

    def one_expert(pieces):
        rows, gate_w, up_w, down_w = pieces
        gate_value = jnp.dot(rows, gate_w, preferred_element_type=jnp.float32)
        up_value = jnp.dot(rows, up_w, preferred_element_type=jnp.float32)
        hidden = (jax.nn.silu(gate_value) * up_value).astype(jnp.bfloat16)
        return jnp.dot(hidden, down_w, preferred_element_type=jnp.float32)
    expert_out = lax.map(one_expert, (expert_rows, gate_full, up_full, down_full))
    per_group = expert_out.reshape(EXPERTS, group_count, CAP, model_width).transpose(1, 0, 2, 3).reshape(group_count, EXPERTS * CAP, model_width)
    routed = jnp.einsum('gtp,gpd->gtd', combiner, per_group, precision=PRECISE).reshape(-1, model_width)
    dense_gate_value = jnp.dot(normed_out, dense_gate, preferred_element_type=jnp.float32)
    dense_up_value = jnp.dot(normed_out, dense_up, preferred_element_type=jnp.float32)
    dense_hidden = (jax.nn.silu(dense_gate_value) * dense_up_value).astype(jnp.bfloat16)
    dense_result = jnp.dot(dense_hidden, dense_down, preferred_element_type=jnp.float32)
    layer_out = (mixed + routed + branch_weight * dense_result).astype(jnp.bfloat16)
    return (layer_out, new_state)
```

```python
import jax
import jax.numpy as jnp
from jax import lax
from jax.sharding import Mesh
from jax.sharding import PartitionSpec as P

RMS_EPSILON = 1e-06
GROUP_EPSILON = 1e-05
PRECISE = lax.Precision.HIGHEST
BF = jnp.bfloat16
F32 = jnp.float32
EP = ("z", "y")
TP = ("x", "c")


def head_decay(head_index, head_total):
    return jnp.exp(
        jnp.log1p(-jnp.exp2(-5.0 - 7.0 * head_index.astype(jnp.float32) / (head_total - 1)))
    )


def rotate_heads(features, positions):
    half_size = features.shape[-1] // 2
    inverse = 10000.0 ** (-jnp.arange(half_size, dtype=jnp.float32) / half_size)
    angles = positions.astype(jnp.float32)[:, None] * inverse[None, :]
    cosine = jnp.cos(angles)[:, None, :]
    sine_part = jnp.sin(angles)[:, None, :]
    first_half = features[..., :half_size]
    second_half = features[..., half_size:]
    return jnp.concatenate(
        [
            first_half * cosine - second_half * sine_part,
            first_half * sine_part + second_half * cosine,
        ],
        axis=-1,
    )


def retention_step(
    normed_in, positions, state, query_weight, key_weight, value_weight, head_index, head_total
):
    row_count, head_count, key_size, value_size = state.shape
    query = jnp.dot(normed_in, query_weight, preferred_element_type=jnp.float32).reshape(
        row_count, head_count, key_size
    )
    keys = jnp.dot(normed_in, key_weight, preferred_element_type=jnp.float32).reshape(
        row_count, head_count, key_size
    )
    values = jnp.dot(normed_in, value_weight, preferred_element_type=jnp.float32).reshape(
        row_count, head_count, value_size
    )
    query = rotate_heads(query, positions)
    keys = rotate_heads(keys, positions) * key_size ** (-0.5)
    decay = head_decay(head_index, head_total)
    new_state = state * decay[None, :, None, None] + keys[:, :, :, None] * values[:, :, None, :]
    retained = jnp.einsum("shk,shkv->shv", query, new_state, precision=PRECISE)
    centered = retained - jnp.mean(retained, axis=-1, keepdims=True)
    normed = centered * lax.rsqrt(
        jnp.mean(centered * centered, axis=-1, keepdims=True) + GROUP_EPSILON
    )
    return (normed.astype(jnp.bfloat16).reshape(row_count, head_count * value_size), new_state)


def padded_halves(w, size):
    return jnp.pad(w, ((0, 2 * size - w.shape[0]), (0, 0))).reshape(2, size, w.shape[1])


def local(
    tokens,
    past_lengths,
    state,
    norm1_gain,
    query_weight,
    key_weight,
    value_weight,
    out_weight,
    norm2_gain,
    branch_gate,
    route_ids,
    route_weights,
    expert_gate,
    expert_up,
    expert_down,
    dense_gate,
    dense_up,
    dense_down,
):
    rows, width = tokens.shape
    x_count = lax.axis_size("x")
    tp_count = 2 * x_count
    ep_count = lax.axis_size(EP)
    tp_index = lax.axis_index(TP)
    blocks = width // 128
    heads_here = state.shape[1]
    head_index = tp_index * heads_here + jnp.arange(heads_here)

    half = -(-dense_gate.shape[1] // 2 // 16) * 16
    part = jnp.concatenate(
        [padded_halves(dense_gate.T, half), padded_halves(dense_up.T, half), padded_halves(dense_down, half)],
        axis=1,
    )
    sent = jnp.broadcast_to(part[None], (x_count, *part.shape)).reshape(tp_count, 3 * half, 128)
    dense_parts = lax.all_to_all(sent, TP, 0, 0, tiled=True)

    inputs = tokens.astype(F32)
    normed_in = (
        inputs
        * lax.rsqrt(jnp.mean(inputs * inputs, axis=-1, keepdims=True) + RMS_EPSILON)
        * norm1_gain
    ).astype(BF)
    normed, new_state = retention_step(
        normed_in,
        past_lengths,
        state,
        query_weight,
        key_weight,
        value_weight,
        head_index,
        heads_here * tp_count,
    )
    partial_mix = jnp.dot(normed, out_weight, preferred_element_type=F32)
    other = lax.ppermute(partial_mix, "c", [(0, 1), (1, 0)])
    pair = (partial_mix + other).astype(BF)
    pair = pair.reshape(rows, blocks, 128).transpose(1, 0, 2).reshape(blocks * rows, 128)
    pairs = lax.all_to_all(
        jnp.broadcast_to(pair[None], (x_count, *pair.shape)), "x", 0, 0, tiled=True
    )
    mix = jnp.sum(pairs.astype(F32), axis=0).reshape(blocks, rows, 128)
    mixed = inputs.reshape(rows, blocks, 128).transpose(1, 0, 2) + mix
    scale = lax.rsqrt(jnp.sum(mixed * mixed, axis=(0, 2), keepdims=True) / width + RMS_EPSILON)
    scaled = mixed * scale * norm2_gain.reshape(blocks, 1, 128)
    branch = jax.nn.sigmoid(jnp.sum(scaled * branch_gate.reshape(blocks, 1, 128), axis=(0, 2)))
    normed_out = scaled.astype(BF).transpose(1, 0, 2).reshape(rows, width)

    expert_count = ep_count // 4
    route_count = route_ids.shape[1]
    route_flat = route_ids.reshape(-1)
    onehot = (route_flat[:, None] == jnp.arange(expert_count, dtype=jnp.int32)[None, :]).astype(
        jnp.int32
    )
    earlier = jnp.cumsum(onehot, axis=0) - onehot
    slot_index = jnp.sum(earlier * onehot, axis=1)
    row_number = jnp.arange(3 * ep_count, dtype=jnp.int32)
    row_expert = row_number // 3 // 4
    row_slot = row_number % 3
    hit = (route_flat[:, None] == row_expert[None, :]) & (slot_index[:, None] == row_slot[None, :])
    hit = hit.astype(F32).reshape(rows, route_count, 3 * ep_count)
    dense_row = (
        (jnp.arange(rows, dtype=jnp.int32)[:, None] == tp_index // 2) & (row_slot[None, :] == 2)
    ).astype(F32)
    selector = (jnp.sum(hit, axis=1) + dense_row).T.astype(BF)
    combiner = jnp.sum(hit * route_weights[:, :, None], axis=1) + dense_row * branch[:, None]

    outgoing = jnp.dot(selector, normed_out, preferred_element_type=F32).astype(BF)
    arrived = lax.all_to_all(
        outgoing.reshape(ep_count, 3 * blocks, 128), EP, 0, 0, tiled=True
    ).reshape(3 * ep_count, width)
    gate_value = jnp.dot(arrived, expert_gate[0], preferred_element_type=F32)
    up_value = jnp.dot(arrived, expert_up[0], preferred_element_type=F32)
    is_dense = (row_slot == 2)[:, None]
    hidden = jnp.where(is_dense, 0.0, jax.nn.silu(gate_value) * up_value).astype(BF)
    gate_t = dense_parts[:, :half].transpose(1, 0, 2).reshape(half, width)
    up_t = dense_parts[:, half : 2 * half].transpose(1, 0, 2).reshape(half, width)
    down = dense_parts[:, 2 * half :].transpose(1, 0, 2).reshape(half, width)
    across = (((1,), (1,)), ((), ()))
    dense_gate_value = lax.dot_general(arrived, gate_t, across, preferred_element_type=F32)
    dense_up_value = lax.dot_general(arrived, up_t, across, preferred_element_type=F32)
    dense_hidden = jnp.where(
        is_dense, jax.nn.silu(dense_gate_value) * dense_up_value, 0.0
    ).astype(BF)
    result = jnp.dot(hidden, expert_down[0], preferred_element_type=F32) + jnp.dot(
        dense_hidden, down, preferred_element_type=F32
    )
    returned = lax.all_to_all(
        result.astype(BF).reshape(ep_count, 3 * blocks, 128), EP, 0, 0, tiled=True
    ).reshape(3 * ep_count, width)
    total = jnp.dot(combiner, returned.astype(F32), precision=PRECISE, preferred_element_type=F32)
    total = total.reshape(rows, blocks, 128).transpose(1, 0, 2).astype(BF)
    sums = lax.all_to_all(total, TP, 0, 0, tiled=True)
    own = lax.dynamic_index_in_dim(mixed, tp_index, 0, keepdims=False)
    layer_out = (own + jnp.sum(sums.astype(F32), axis=0)).astype(BF)
    return (layer_out, new_state)


def solution(mesh):
    split = Mesh(mesh.devices.reshape(8, 8, 8, 2), ("z", "y", "x", "c"))
    return jax.shard_map(
        local,
        mesh=split,
        in_specs=(
            P(EP, None),
            P(EP),
            P(EP, TP, None, None),
            P(),
            P(None, TP),
            P(None, TP),
            P(None, TP),
            P(TP, None),
            P(),
            P(),
            P(EP, None),
            P(EP, None),
            P(EP, None, TP),
            P(EP, None, TP),
            P(EP, TP, None),
            P(TP, EP),
            P(TP, EP),
            P(EP, TP),
        ),
        out_specs=(P(EP, TP), P(EP, TP, None, None)),
        check_vma=False,
    )
```

```python
import jax
import jax.numpy as jnp
from jax import lax
from jax.experimental import pallas as pl
from jax.experimental.pallas import tpu as pltpu
from jax.sharding import Mesh
from jax.sharding import PartitionSpec as P

RMS_EPSILON = 1e-06
GROUP_EPSILON = 1e-05
BF = jnp.bfloat16
F32 = jnp.float32
EP = ("z", "y")
TP = ("x", "c")
NT = (((1,), (1,)), ((), ()))


def padded_halves(w, size):
    return jnp.pad(w, ((0, 2 * size - w.shape[0]), (0, 0))).reshape(2, size, w.shape[1])


def call(kernel, out_shape, args, flops, scratch=(), specs=None, out_specs=None, vmem=None):
    full = pl.BlockSpec(memory_space=pltpu.VMEM)
    size = sum(a.size * a.dtype.itemsize for a in args)
    return pl.pallas_call(
        kernel,
        out_shape=out_shape,
        in_specs=specs or [full] * len(args),
        out_specs=out_specs or jax.tree.map(lambda _: full, out_shape),
        scratch_shapes=list(scratch),
        compiler_params=pltpu.CompilerParams(vmem_limit_bytes=vmem or 16 << 20),
        cost_estimate=pl.CostEstimate(flops=flops, bytes_accessed=size, transcendentals=0),
    )(*args)


def retention_kernel(
    core_ref,
    tokens_ref,
    gain_ref,
    cos_ref,
    sin_ref,
    decay_ref,
    q_hbm,
    k_hbm,
    v_hbm,
    state_hbm,
    out_hbm,
    keep_ref,
    give_ref,
    new_hbm,
    q_w,
    k_w,
    v_w,
    state,
    out_w,
    fresh,
    sems,
):
    rows, width = tokens_ref.shape
    copies = [
        pltpu.make_async_copy(s, d, sems.at[n])
        for n, (s, d) in enumerate(
            ((q_hbm, q_w), (k_hbm, k_w), (v_hbm, v_w), (state_hbm, state), (out_hbm, out_w))
        )
    ]
    for c in copies:
        c.start()
    x = tokens_ref[...].astype(F32)
    inv = lax.rsqrt(jnp.sum(x * x, axis=1, keepdims=True) / width + RMS_EPSILON)
    normed_in = (x * inv * gain_ref[...]).astype(BF)

    def project(n, w):
        copies[n].wait()
        return jnp.dot(normed_in, w[...], preferred_element_type=F32)

    def rotated(v):
        return v * cos_ref[...] + pltpu.roll(v, v.shape[1] // 2, 1) * sin_ref[...]

    query = rotated(project(0, q_w))
    keys = rotated(project(1, k_w)) * q_w.shape[1] ** (-0.5)
    values = project(2, v_w)
    query_t = query.T
    keys_t = keys.T
    copies[3].wait()
    decay = decay_ref[0]
    retained = []
    for i in range(rows):
        new = state[i] * decay + keys_t[:, i : i + 1] * values[i : i + 1, :]
        fresh[i] = new
        retained.append(jnp.sum(query_t[:, i : i + 1] * new, axis=0, keepdims=True))
    back = pltpu.make_async_copy(fresh, new_hbm, sems.at[5])
    back.start()
    retained = jnp.concatenate(retained, axis=0)
    centered = retained - jnp.mean(retained, axis=1, keepdims=True)
    normed = centered * lax.rsqrt(
        jnp.mean(centered * centered, axis=1, keepdims=True) + GROUP_EPSILON
    )
    normed = normed.astype(BF)
    copies[4].wait()
    mix = jnp.dot(normed, out_w[...], preferred_element_type=F32)
    for j in range(width // 128):
        keep_ref[j] = mix[:, 128 * j : 128 * j + 128]
        give_ref[j] = mix[:, 128 * j : 128 * j + 128].astype(BF)
    back.wait()


def dispatch_kernel(
    core_ref, pairs_ref, tokens_ref, gain_ref, gate_ref, select_ref, sent_ref, own_ref, branch_ref, held
):
    rows, width = tokens_ref.shape
    blocks = width // 128
    square = jnp.zeros((rows, 128), F32)
    for j in range(blocks):
        m = tokens_ref[:, 128 * j : 128 * j + 128].astype(F32)
        for p in range(pairs_ref.shape[0]):
            m = m + pairs_ref[p, j].astype(F32)
        held[j] = m
        square = square + m * m
    scale = lax.rsqrt(jnp.sum(square, axis=1, keepdims=True) / width + RMS_EPSILON)
    along = jnp.zeros((rows, 128), F32)
    for j in range(blocks):
        along = along + held[j] * scale * gain_ref[j : j + 1, :] * gate_ref[j : j + 1, :]
    branch_ref[...] = jax.nn.sigmoid(
        jnp.broadcast_to(jnp.sum(along, axis=1, keepdims=True), (rows, 128))
    )
    core = core_ref[1]
    own_ref[...] = held[core_ref[0]]
    mine = [
        held[2 * k + core] * scale * gain_ref[pl.ds(2 * k + core, 1), :] for k in range(blocks // 2)
    ]
    mine = jnp.concatenate(mine, axis=0).astype(BF)
    sent_ref[...] = jnp.dot(select_ref[...], mine, preferred_element_type=F32).astype(BF)


def expert_kernel(
    core_ref,
    mine_ref,
    other_ref,
    gate_ref,
    up_ref,
    down_ref,
    dense_ref,
    keep_ref,
    give_ref,
):
    count, half_width = mine_ref.shape
    half = dense_ref.shape[1] // 3
    core = core_ref[1]
    wide = gate_ref.shape[0]
    gate = jnp.zeros((count, wide), F32)
    up = jnp.zeros((count, wide), F32)
    dense = jnp.zeros((count, 2 * half), F32)
    for ref, parity in ((mine_ref, core), (other_ref, 1 - core)):
        for k in range(half_width // 128):
            x = ref[:, 128 * k : 128 * k + 128]
            at = pl.ds(pl.multiple_of((2 * k + parity) * 128, 128), 128)
            gate = gate + lax.dot_general(x, gate_ref[:, at], NT, preferred_element_type=F32)
            up = up + lax.dot_general(x, up_ref[:, at], NT, preferred_element_type=F32)
            dense = dense + lax.dot_general(
                x, dense_ref[2 * k + parity, : 2 * half, :], NT, preferred_element_type=F32
            )
    is_dense = lax.broadcasted_iota(jnp.int32, (count, 1), 0) % 3 == 2
    hidden = (gate / (1.0 + jnp.exp(-gate))) * up
    hidden = jnp.where(is_dense, 0.0, hidden).astype(BF)
    dgate = dense[:, :half]
    dense_hidden = (dgate / (1.0 + jnp.exp(-dgate))) * dense[:, half:]
    dense_hidden = jnp.where(is_dense, dense_hidden, 0.0).astype(BF)
    for out, parity in ((keep_ref, core), (give_ref, 1 - core)):
        for k in range(half_width // 128):
            at = pl.ds(pl.multiple_of((2 * k + parity) * 128, 128), 128)
            r = jnp.dot(hidden, down_ref[:, at], preferred_element_type=F32)
            r = r + jnp.dot(
                dense_hidden, dense_ref[2 * k + parity, 2 * half :, :], preferred_element_type=F32
            )
            out[:, 128 * k : 128 * k + 128] = r.astype(out.dtype)


def combine_kernel(high_ref, low_ref, back_ref, out_ref):
    back = back_ref[...]
    out_ref[...] = (
        jnp.dot(high_ref[...], back, preferred_element_type=F32)
        + jnp.dot(low_ref[...], back, preferred_element_type=F32)
    ).astype(BF)


def swap(x):
    return lax.ppermute(x, "c", [(0, 1), (1, 0)])


def local(
    tokens,
    past_lengths,
    state,
    norm1_gain,
    query_weight,
    key_weight,
    value_weight,
    out_weight,
    norm2_gain,
    branch_gate,
    route_ids,
    route_weights,
    expert_gate,
    expert_up,
    expert_down,
    dense_gate,
    dense_up,
    dense_down,
):
    rows, width = tokens.shape
    x_count = lax.axis_size("x")
    tp_count = 2 * x_count
    ep_count = lax.axis_size(EP)
    x_index = lax.axis_index("x")
    tp_index = lax.axis_index(TP)
    blocks = width // 128
    key_size = query_weight.shape[1]
    value_size = value_weight.shape[1]
    place = jnp.stack([tp_index, lax.axis_index("c")]).astype(jnp.int32)
    smem = pl.BlockSpec(memory_space=pltpu.SMEM)
    vmem = pl.BlockSpec(memory_space=pltpu.VMEM)
    hbm = pl.BlockSpec(memory_space=pltpu.HBM)

    half = -(-dense_gate.shape[1] // 2 // 16) * 16
    part = jnp.concatenate(
        [
            padded_halves(dense_gate.T, half),
            padded_halves(dense_up.T, half),
            padded_halves(dense_down, half),
        ],
        axis=1,
    )
    sent = jnp.broadcast_to(part[None], (x_count, *part.shape)).reshape(tp_count, 3 * half, 128)
    dense_parts = lax.all_to_all(sent, TP, 0, 0, tiled=True)

    inverse = 10000.0 ** (-jnp.arange(key_size // 2, dtype=F32) / (key_size // 2))
    angles = past_lengths.astype(F32)[:, None] * inverse[None, :]
    cosine, sine = jnp.cos(angles), jnp.sin(angles)
    cosine = jnp.concatenate([cosine, cosine], axis=1)
    sine = jnp.concatenate([-sine, sine], axis=1)
    decay = jnp.exp(jnp.log1p(-jnp.exp2(-5.0 - 7.0 * tp_index.astype(F32) / (tp_count - 1))))
    args = (
        place,
        tokens,
        norm1_gain.reshape(1, width),
        cosine,
        sine,
        decay.reshape(1),
        query_weight,
        key_weight,
        value_weight,
        state.reshape(rows, key_size, value_size),
        out_weight,
    )
    keep, give, new_state = call(
        retention_kernel,
        (
            jax.ShapeDtypeStruct((blocks, rows, 128), F32),
            jax.ShapeDtypeStruct((blocks, rows, 128), BF),
            jax.ShapeDtypeStruct((rows, key_size, value_size), F32),
        ),
        args,
        10_000_000_000,
        scratch=(
            pltpu.VMEM(query_weight.shape, BF),
            pltpu.VMEM(key_weight.shape, BF),
            pltpu.VMEM(value_weight.shape, BF),
            pltpu.VMEM((rows, key_size, value_size), F32),
            pltpu.VMEM(out_weight.shape, BF),
            pltpu.VMEM((rows, key_size, value_size), F32),
            pltpu.SemaphoreType.DMA((6,)),
        ),
        specs=[smem, vmem, vmem, vmem, vmem, smem, hbm, hbm, hbm, hbm, hbm],
        out_specs=(vmem, vmem, hbm),
        vmem=61 << 20,
    )
    pair = (keep + swap(give).astype(F32)).astype(BF)
    pairs = lax.all_to_all(
        jnp.broadcast_to(pair[None], (x_count, *pair.shape)), "x", 0, 0, tiled=True
    )

    route_count = route_ids.shape[1]
    route_flat = route_ids.reshape(-1)
    same = (route_flat[:, None] == route_flat[None, :]).astype(jnp.int32)
    number = jnp.arange(rows * route_count, dtype=jnp.int32)
    slot_index = jnp.sum(same * (number[None, :] < number[:, None]), axis=1)
    place_of = jnp.where(slot_index < 2, route_flat * 3 + slot_index, -1)
    in_row = lax.broadcasted_iota(jnp.int32, (3 * ep_count, 1), 0)
    row_kind = (in_row // 12) * 3 + in_row % 3
    hit = (row_kind == place_of[None, :]).astype(F32).reshape(3 * ep_count, rows, route_count)
    dense_row = (
        (jnp.arange(rows, dtype=jnp.int32)[None, :] == x_index) & (in_row % 3 == 2)
    ).astype(F32)
    chosen = jnp.sum(hit, axis=2) + dense_row
    weighted = jnp.sum(hit * route_weights[None], axis=2)
    ones = jnp.eye(blocks // 2, dtype=F32)
    select = (chosen[:, None, None, :] * ones[None, :, :, None]).astype(BF)
    select = select.reshape(3 * ep_count * blocks // 2, blocks // 2 * rows)

    args = (
        place,
        pairs,
        tokens,
        norm2_gain.reshape(blocks, 128),
        branch_gate.reshape(blocks, 128),
        select,
    )
    outgoing, own, branch = call(
        dispatch_kernel,
        (
            jax.ShapeDtypeStruct((select.shape[0], 128), BF),
            jax.ShapeDtypeStruct((rows, 128), F32),
            jax.ShapeDtypeStruct((rows, 128), F32),
        ),
        args,
        1_000_000_000,
        specs=[smem] + [vmem] * 5,
        scratch=(pltpu.VMEM((blocks, rows, 128), F32),),
    )
    arrived = lax.all_to_all(outgoing.reshape(ep_count, 3 * blocks // 2, 128), EP, 0, 0, tiled=True)
    mine = arrived.reshape(3 * ep_count, width // 2)
    other = swap(mine)
    args = (
        place,
        mine,
        other,
        expert_gate[0].T,
        expert_up[0].T,
        expert_down[0],
        dense_parts,
    )
    shape = (3 * ep_count, width // 2)
    stay, leave = call(
        expert_kernel,
        (jax.ShapeDtypeStruct(shape, F32), jax.ShapeDtypeStruct(shape, BF)),
        args,
        2_000_000_000,
        specs=[smem] + [vmem] * 6,
    )
    result = (stay + swap(leave).astype(F32)).astype(BF)
    returned = lax.all_to_all(result.reshape(ep_count, 3 * blocks // 2, 128), EP, 0, 0, tiled=True)
    combiner = weighted + dense_row * branch[:, 0][None, :]
    spread = combiner.T[None, :, :, None] * ones[:, None, None, :]
    spread = spread.reshape(blocks // 2 * rows, 3 * ep_count * blocks // 2)
    high = lax.reduce_precision(spread, 8, 7)
    low = (spread - high).astype(BF)
    total = call(
        combine_kernel,
        jax.ShapeDtypeStruct((blocks // 2 * rows, 128), BF),
        (high.astype(BF), low, returned.reshape(3 * ep_count * blocks // 2, 128)),
        100_000_000,
    )
    sums = lax.all_to_all(total.reshape(x_count, rows, 128), "x", 0, 0, tiled=True)
    layer_out = (own + jnp.sum(sums.astype(F32), axis=0)).astype(BF)
    return (layer_out, new_state.reshape(state.shape))


def solution(mesh):
    split = Mesh(mesh.devices.reshape(8, 8, 8, 2), ("z", "y", "x", "c"))
    return jax.shard_map(
        local,
        mesh=split,
        in_specs=(
            P(EP, None),
            P(EP),
            P(EP, TP, None, None),
            P(),
            P(None, TP),
            P(None, TP),
            P(None, TP),
            P(TP, None),
            P(),
            P(),
            P(EP, None),
            P(EP, None),
            P(EP, None, TP),
            P(EP, None, TP),
            P(EP, TP, None),
            P(TP, EP),
            P(TP, EP),
            P(EP, TP),
        ),
        out_specs=(P(EP, TP), P(EP, TP, None, None)),
        check_vma=False,
    )
```

```python
import jax
import jax.numpy as jnp
from jax import lax
from jax.experimental import pallas as pl
from jax.experimental.pallas import tpu as pltpu
from jax.sharding import Mesh
from jax.sharding import PartitionSpec as P

RMS_EPSILON = 1e-06
GROUP_EPSILON = 1e-05
BF = jnp.bfloat16
F32 = jnp.float32
EP = ("z", "y")
TP = ("x", "c")
NT = (((1,), (1,)), ((), ()))
FULL = 61 << 20


def call(kernel, out_shape, args, flops, scratch=(), specs=None, out_specs=None, vmem=None):
    full = pl.BlockSpec(memory_space=pltpu.VMEM)
    size = sum(a.size * a.dtype.itemsize for a in args)
    return pl.pallas_call(
        kernel,
        out_shape=out_shape,
        in_specs=specs or [full] * len(args),
        out_specs=out_specs or jax.tree.map(lambda _: full, out_shape),
        scratch_shapes=list(scratch),
        compiler_params=pltpu.CompilerParams(vmem_limit_bytes=vmem or 16 << 20),
        cost_estimate=pl.CostEstimate(flops=flops, bytes_accessed=size, transcendentals=0),
    )(*args)


def regroup_kernel(gate_hbm, up_hbm, down_hbm, sent_hbm, parts, packed, sems):
    half = packed.shape[1] // 3
    size = gate_hbm.shape[0]
    count = sent_hbm.shape[0]
    copies = [
        pltpu.make_async_copy(ref, parts.at[n], sems.at[count + n])
        for n, ref in enumerate((gate_hbm, up_hbm, down_hbm))
    ]
    for c in copies:
        c.start()
    for n in range(3):
        packed[1, half * n + size - half : half * n + half, :] = jnp.zeros(
            (2 * half - size, packed.shape[2]), BF
        )
    for n, c in enumerate(copies):
        c.wait()
        packed[0, half * n : half * n + half, :] = parts[n, :half, :]
        packed[1, half * n : half * n + size - half, :] = parts[n, half:, :]
    copies = [pltpu.make_async_copy(packed, sent_hbm.at[n], sems.at[n]) for n in range(count)]
    for c in copies:
        c.start()
    for c in copies:
        c.wait()


def retention_kernel(
    tokens_ref,
    gain_ref,
    cos_ref,
    sin_ref,
    decay_ref,
    q_hbm,
    k_hbm,
    v_hbm,
    state_hbm,
    out_hbm,
    keep_ref,
    give_ref,
    new_hbm,
    q_w,
    k_w,
    v_w,
    state,
    out_w,
    fresh,
    held,
    sems,
):
    rows, width = tokens_ref.shape
    core = lax.axis_index("c")
    copies = [
        pltpu.make_async_copy(s, d, sems.at[n])
        for n, (s, d) in enumerate(
            ((q_hbm, q_w), (k_hbm, k_w), (v_hbm, v_w), (state_hbm, state), (out_hbm, out_w))
        )
    ]
    for c in copies:
        c.start()
    x = tokens_ref[...].astype(F32)
    inv = lax.rsqrt(jnp.sum(x * x, axis=1, keepdims=True) / width + RMS_EPSILON)
    normed_in = (x * inv * gain_ref[...]).astype(BF)

    def project(n, w):
        copies[n].wait()
        return jnp.dot(normed_in, w[...], preferred_element_type=F32)

    def rotated(v):
        return v * cos_ref[...] + pltpu.roll(v, v.shape[1] // 2, 1) * sin_ref[...]

    query = rotated(project(0, q_w))
    keys = rotated(project(1, k_w)) * q_w.shape[1] ** (-0.5)
    values = project(2, v_w)
    query_t = query.T
    keys_t = keys.T
    copies[3].wait()
    decay = decay_ref[0]
    retained = []
    for i in range(rows):
        new = state[i] * decay + keys_t[:, i : i + 1] * values[i : i + 1, :]
        fresh[i] = new
        retained.append(jnp.sum(query_t[:, i : i + 1] * new, axis=0, keepdims=True))
    back = pltpu.make_async_copy(fresh, new_hbm, sems.at[5])
    back.start()
    retained = jnp.concatenate(retained, axis=0)
    centered = retained - jnp.mean(retained, axis=1, keepdims=True)
    normed = centered * lax.rsqrt(
        jnp.mean(centered * centered, axis=1, keepdims=True) + GROUP_EPSILON
    )
    normed = normed.astype(BF)
    copies[4].wait()
    mix = jnp.dot(normed, out_w[...], preferred_element_type=F32)
    for j in range(width // 128):
        held[j] = mix[:, 128 * j : 128 * j + 128]
    for k in range(width // 256):
        keep_ref[k] = held[2 * k + core]
        give_ref[k] = held[2 * k + 1 - core].astype(BF)
    back.wait()


def pair_kernel(keep_ref, got_ref, sent_hbm, pair, sems):
    pair[...] = (keep_ref[...] + got_ref[...].astype(F32)).astype(BF)
    copies = [
        pltpu.make_async_copy(pair, sent_hbm.at[n], sems.at[n]) for n in range(sent_hbm.shape[0])
    ]
    for c in copies:
        c.start()
    for c in copies:
        c.wait()


def dispatch_kernel(
    pairs_ref, tokens_ref, gain_ref, gate_ref, select_ref, sent_ref, own_ref, stat_ref, held
):
    rows = tokens_ref.shape[0]
    blocks = pairs_ref.shape[1]
    core = lax.axis_index("c")
    square = jnp.zeros((rows, 128), F32)
    along = jnp.zeros((rows, 128), F32)
    mine = []
    for k in range(blocks):
        j = 2 * k + core
        m = tokens_ref[:, pl.ds(pl.multiple_of(j * 128, 128), 128)].astype(F32)
        for p in range(pairs_ref.shape[0]):
            m = m + pairs_ref[p, k].astype(F32)
        held[k] = m
        square = square + m * m
        along = along + m * gain_ref[pl.ds(j, 1), :] * gate_ref[pl.ds(j, 1), :]
        mine.append(m)
    own_ref[...] = held[lax.axis_index("x")]
    lane = lax.broadcasted_iota(jnp.int32, (rows, 128), 1)
    stat_ref[...] = jnp.where(
        lane < 64, jnp.sum(square, axis=1, keepdims=True), jnp.sum(along, axis=1, keepdims=True)
    )
    mine = jnp.concatenate(mine, axis=0).astype(BF)
    count, _, wide = select_ref.shape
    same = lax.broadcasted_iota(jnp.int32, (blocks, wide), 0) == (
        lax.broadcasted_iota(jnp.int32, (blocks, wide), 1) // rows
    )
    spread = jnp.broadcast_to(select_ref[...], (count, blocks, wide)) * same.astype(F32)[None]
    spread = spread.reshape(count * blocks, wide).astype(BF)
    sent_ref[...] = jnp.dot(spread, mine, preferred_element_type=F32).astype(BF)


def expert_kernel(
    mine_ref, other_ref, gain_ref, gate_ref, up_ref, down_ref, dense_ref, keep_ref, give_ref
):
    count, half_width = mine_ref.shape
    blocks = half_width // 128
    half = dense_ref.shape[1] // 3
    core = lax.axis_index("c")
    sides = ((mine_ref, core), (other_ref, 1 - core))

    def columns(ref, parity):
        return jnp.concatenate(
            [
                ref[:, pl.ds(pl.multiple_of((2 * k + parity) * 128, 128), 128)]
                for k in range(blocks)
            ],
            axis=1,
        )

    def dense_columns(parity, low, high):
        return jnp.concatenate(
            [dense_ref[2 * k + parity, low:high, :] for k in range(blocks)], axis=1
        )

    square = jnp.zeros((count, 128), F32)
    for ref, _ in sides:
        for k in range(blocks):
            x = ref[:, 128 * k : 128 * k + 128].astype(F32)
            square = square + x * x
    scale = lax.rsqrt(
        jnp.sum(square, axis=1, keepdims=True) / (2 * half_width) + RMS_EPSILON
    )
    gate = up = dense = 0.0
    for ref, parity in sides:
        x = jnp.concatenate(
            [
                (
                    ref[:, 128 * k : 128 * k + 128].astype(F32)
                    * scale
                    * gain_ref[pl.ds(2 * k + parity, 1), :]
                ).astype(BF)
                for k in range(blocks)
            ],
            axis=1,
        )

        def along(w):
            return lax.dot_general(x, w, NT, preferred_element_type=F32)

        gate = gate + along(columns(gate_ref, parity))
        up = up + along(columns(up_ref, parity))
        dense = dense + along(dense_columns(parity, 0, 2 * half))
    is_dense = lax.broadcasted_iota(jnp.int32, (count, 1), 0) % 3 == 2
    hidden = (gate / (1.0 + jnp.exp(-gate))) * up
    hidden = jnp.where(is_dense, 0.0, hidden).astype(BF)
    dense_gate = dense[:, :half]
    dense_hidden = (dense_gate / (1.0 + jnp.exp(-dense_gate))) * dense[:, half:]
    dense_hidden = jnp.where(is_dense, dense_hidden, 0.0).astype(BF)
    for out, parity in ((give_ref, 1 - core), (keep_ref, core)):
        r = jnp.dot(hidden, columns(down_ref, parity), preferred_element_type=F32)
        r = r + jnp.dot(
            dense_hidden, dense_columns(parity, 2 * half, 3 * half), preferred_element_type=F32
        )
        out[...] = r.astype(out.dtype)


def combine_kernel(weight_ref, mine_ref, other_ref, back_ref, out_ref):
    rows, count = weight_ref.shape
    blocks = out_ref.shape[0]
    stat = mine_ref[...] + other_ref[...]
    scale = lax.rsqrt(stat[:, :1] / (2 * blocks * 128) + RMS_EPSILON)
    branch = jax.nn.sigmoid(scale * stat[:, 64:65])
    row = lax.broadcasted_iota(jnp.int32, (rows, count), 0)
    place = lax.broadcasted_iota(jnp.int32, (rows, count), 1)
    dense = (row == lax.axis_index("x")) & (place % 3 == 2)
    weight = jnp.where(dense, branch, weight_ref[...])
    high = weight.astype(BF)
    low = (weight - high.astype(F32)).astype(BF)
    back = back_ref[...]
    total = jnp.dot(high, back, preferred_element_type=F32) + jnp.dot(
        low, back, preferred_element_type=F32
    )
    for k in range(blocks):
        out_ref[k] = total[:, 128 * k : 128 * k + 128]


def swap(x):
    return lax.ppermute(x, "c", [(0, 1), (1, 0)])


def local(
    tokens,
    past_lengths,
    state,
    norm1_gain,
    query_weight,
    key_weight,
    value_weight,
    out_weight,
    norm2_gain,
    branch_gate,
    route_ids,
    route_weights,
    expert_gate,
    expert_up,
    expert_down,
    dense_gate,
    dense_up,
    dense_down,
):
    rows, width = tokens.shape
    x_count = lax.axis_size("x")
    tp_count = 2 * x_count
    ep_count = lax.axis_size(EP)
    x_index = lax.axis_index("x")
    tp_index = lax.axis_index(TP)
    blocks = width // 128
    own_blocks = blocks // 2
    key_size = query_weight.shape[1]
    value_size = value_weight.shape[1]
    smem = pl.BlockSpec(memory_space=pltpu.SMEM)
    vmem = pl.BlockSpec(memory_space=pltpu.VMEM)
    hbm = pl.BlockSpec(memory_space=pltpu.HBM)
    shaped = jax.ShapeDtypeStruct

    half = -(-dense_gate.shape[1] // 2 // 16) * 16
    sent = call(
        regroup_kernel,
        shaped((x_count, 2, 3 * half, 128), BF),
        (dense_gate.T, dense_up.T, dense_down),
        1_000_000,
        scratch=(
            pltpu.VMEM((3, *dense_down.shape), BF),
            pltpu.VMEM((2, 3 * half, 128), BF),
            pltpu.SemaphoreType.DMA((x_count + 3,)),
        ),
        specs=[hbm, hbm, hbm],
        out_specs=hbm,
        vmem=FULL,
    )
    dense_parts = lax.all_to_all(
        sent.reshape(tp_count, 3 * half, 128), TP, 0, 0, tiled=True
    )

    lane = jnp.arange(key_size, dtype=jnp.int32)
    inverse = 10000.0 ** (-(lane % (key_size // 2)).astype(F32) / (key_size // 2))
    angles = past_lengths.astype(F32)[:, None] * inverse[None, :]
    cosine = jnp.cos(angles)
    sine = jnp.sin(angles) * jnp.where(lane < key_size // 2, -1.0, 1.0)[None, :]
    decay = jnp.exp(jnp.log1p(-jnp.exp2(-5.0 - 7.0 * tp_index.astype(F32) / (tp_count - 1))))
    keep, give, new_state = call(
        retention_kernel,
        (
            shaped((own_blocks, rows, 128), F32),
            shaped((own_blocks, rows, 128), BF),
            shaped((rows, key_size, value_size), F32),
        ),
        (
            tokens,
            norm1_gain.reshape(1, width),
            cosine,
            sine,
            decay.reshape(1),
            query_weight,
            key_weight,
            value_weight,
            state.reshape(rows, key_size, value_size),
            out_weight,
        ),
        10_000_000_000,
        scratch=(
            pltpu.VMEM(query_weight.shape, BF),
            pltpu.VMEM(key_weight.shape, BF),
            pltpu.VMEM(value_weight.shape, BF),
            pltpu.VMEM((rows, key_size, value_size), F32),
            pltpu.VMEM(out_weight.shape, BF),
            pltpu.VMEM((rows, key_size, value_size), F32),
            pltpu.VMEM((blocks, rows, 128), F32),
            pltpu.SemaphoreType.DMA((6,)),
        ),
        specs=[vmem, vmem, vmem, vmem, smem, hbm, hbm, hbm, hbm, hbm],
        out_specs=(vmem, vmem, hbm),
        vmem=FULL,
    )
    sent = call(
        pair_kernel,
        shaped((x_count, own_blocks, rows, 128), BF),
        (keep, swap(give)),
        1_000_000,
        scratch=(
            pltpu.VMEM((own_blocks, rows, 128), BF),
            pltpu.SemaphoreType.DMA((x_count,)),
        ),
        out_specs=hbm,
    )
    pairs = lax.all_to_all(sent, "x", 0, 0, tiled=True)

    route_count = route_ids.shape[1]
    route_flat = route_ids.reshape(-1)
    same = (route_flat[:, None] == route_flat[None, :]).astype(jnp.int32)
    number = jnp.arange(rows * route_count, dtype=jnp.int32)
    slot_index = jnp.sum(same * (number[None, :] < number[:, None]), axis=1)
    place_of = jnp.where(slot_index < 2, route_flat * 3 + slot_index, -1)
    place_of = place_of.reshape(rows, route_count)
    in_row = jnp.arange(3 * ep_count, dtype=jnp.int32)
    row_kind = (in_row // 12) * 3 + in_row % 3
    weighted = jnp.sum(
        jnp.where(place_of[:, :, None] == row_kind, route_weights[:, :, None], 0.0), axis=1
    )
    token = jnp.arange(own_blocks * rows, dtype=jnp.int32) % rows
    tiled = jnp.tile(place_of, (own_blocks, 1))
    chosen = jnp.any(tiled[None] == row_kind[:, None, None], axis=2) | (
        (in_row[:, None] % 3 == 2) & (token[None, :] == x_index)
    )
    select = chosen.astype(F32)[:, None, :]

    outgoing, own, stat = call(
        dispatch_kernel,
        (
            shaped((3 * ep_count * own_blocks, 128), BF),
            shaped((rows, 128), F32),
            shaped((rows, 128), F32),
        ),
        (pairs, tokens, norm2_gain.reshape(blocks, 128), branch_gate.reshape(blocks, 128), select),
        1_000_000_000,
        scratch=(pltpu.VMEM((own_blocks, rows, 128), F32),),
    )
    arrived = lax.all_to_all(outgoing.reshape(ep_count, 3 * own_blocks, 128), EP, 0, 0, tiled=True)
    other_stat = swap(stat)
    mine = arrived.reshape(3 * ep_count, width // 2)
    other = swap(mine)
    shape = (3 * ep_count, width // 2)
    stay, leave = call(
        expert_kernel,
        (shaped(shape, F32), shaped(shape, BF)),
        (
            mine,
            other,
            norm2_gain.reshape(blocks, 128),
            expert_gate[0].T,
            expert_up[0].T,
            expert_down[0],
            dense_parts,
        ),
        2_000_000_000,
    )
    result = (stay + swap(leave).astype(F32)).astype(BF)
    returned = lax.all_to_all(result.reshape(ep_count, 3 * own_blocks, 128), EP, 0, 0, tiled=True)
    total = call(
        combine_kernel,
        shaped((own_blocks, rows, 128), F32),
        (weighted, stat, other_stat, returned.reshape(3 * ep_count, width // 2)),
        100_000_000,
    )
    sums = lax.all_to_all(total, "x", 0, 0, tiled=True)
    layer_out = (own + jnp.sum(sums, axis=0)).astype(BF)
    return (layer_out, new_state.reshape(state.shape))


def solution(mesh):
    split = Mesh(mesh.devices.reshape(8, 8, 8, 2), ("z", "y", "x", "c"))
    return jax.shard_map(
        local,
        mesh=split,
        in_specs=(
            P(EP, None),
            P(EP),
            P(EP, TP, None, None),
            P(),
            P(None, TP),
            P(None, TP),
            P(None, TP),
            P(TP, None),
            P(),
            P(),
            P(EP, None),
            P(EP, None),
            P(EP, None, TP),
            P(EP, None, TP),
            P(EP, TP, None),
            P(TP, EP),
            P(TP, EP),
            P(EP, TP),
        ),
        out_specs=(P(EP, TP), P(EP, TP, None, None)),
        check_vma=False,
    )
```

```python
import jax
import jax.numpy as jnp
from jax import lax
from jax.experimental import pallas as pl
from jax.experimental.pallas import tpu as pltpu
from jax.sharding import Mesh
from jax.sharding import PartitionSpec as P

RMS_EPSILON = 1e-06
GROUP_EPSILON = 1e-05
BF = jnp.bfloat16
F32 = jnp.float32
EP = ("z", "y")
TP = ("x", "c")
NT = (((1,), (1,)), ((), ()))
FULL = 61 << 20


def call(kernel, out_shape, args, flops, scratch=(), specs=None, out_specs=None, vmem=None):
    full = pl.BlockSpec(memory_space=pltpu.VMEM)
    size = sum(a.size * a.dtype.itemsize for a in args)
    return pl.pallas_call(
        kernel,
        out_shape=out_shape,
        in_specs=specs or [full] * len(args),
        out_specs=out_specs or jax.tree.map(lambda _: full, out_shape),
        scratch_shapes=list(scratch),
        compiler_params=pltpu.CompilerParams(vmem_limit_bytes=vmem or 16 << 20),
        cost_estimate=pl.CostEstimate(flops=flops, bytes_accessed=size, transcendentals=0),
    )(*args)


def regroup_kernel(gate_hbm, up_hbm, down_hbm, sent_hbm, parts, packed, sems):
    half = gate_hbm.shape[0] // 2
    count = sent_hbm.shape[0]
    copies = [
        pltpu.make_async_copy(ref, parts.at[n], sems.at[count + n])
        for n, ref in enumerate((gate_hbm, up_hbm, down_hbm))
    ]
    for c in copies:
        c.start()
    spare = packed.shape[1] - 3 * half
    for p in range(2):
        packed[p, 3 * half :, :] = jnp.zeros((spare, packed.shape[2]), BF)
    for n, c in enumerate(copies):
        c.wait()
        for p in range(2):
            packed[p, half * n : half * n + half, :] = parts[n, half * p : half * p + half, :]
    copies = [pltpu.make_async_copy(packed, sent_hbm.at[n], sems.at[n]) for n in range(count)]
    for c in copies:
        c.start()
    for c in copies:
        c.wait()


def retention_kernel(
    tokens_ref,
    gain_ref,
    cos_ref,
    sin_ref,
    decay_ref,
    q_hbm,
    k_hbm,
    v_hbm,
    state_hbm,
    out_hbm,
    keep_ref,
    give_ref,
    new_hbm,
    q_w,
    k_w,
    v_w,
    state,
    out_w,
    fresh,
    held,
    sems,
):
    rows, width = tokens_ref.shape
    core = lax.axis_index("c")
    copies = [
        pltpu.make_async_copy(s, d, sems.at[n])
        for n, (s, d) in enumerate(
            ((q_hbm, q_w), (k_hbm, k_w), (v_hbm, v_w), (state_hbm, state), (out_hbm, out_w))
        )
    ]
    for c in copies:
        c.start()
    x = tokens_ref[...].astype(F32)
    inv = lax.rsqrt(jnp.sum(x * x, axis=1, keepdims=True) / width + RMS_EPSILON)
    normed_in = (x * inv * gain_ref[...]).astype(BF)

    def project(n, w):
        copies[n].wait()
        return jnp.dot(normed_in, w[...], preferred_element_type=F32)

    def rotated(v):
        return v * cos_ref[...] + pltpu.roll(v, v.shape[1] // 2, 1) * sin_ref[...]

    query = rotated(project(0, q_w))
    keys = rotated(project(1, k_w)) * q_w.shape[1] ** (-0.5)
    values = project(2, v_w)
    query_t = query.T
    keys_t = keys.T
    copies[3].wait()
    decay = decay_ref[0]
    retained = []
    for i in range(rows):
        new = state[i] * decay + keys_t[:, i : i + 1] * values[i : i + 1, :]
        fresh[i] = new
        retained.append(jnp.sum(query_t[:, i : i + 1] * new, axis=0, keepdims=True))
    back = pltpu.make_async_copy(fresh, new_hbm, sems.at[5])
    back.start()
    retained = jnp.concatenate(retained, axis=0)
    centered = retained - jnp.mean(retained, axis=1, keepdims=True)
    normed = centered * lax.rsqrt(
        jnp.mean(centered * centered, axis=1, keepdims=True) + GROUP_EPSILON
    )
    normed = normed.astype(BF)
    copies[4].wait()
    mix = jnp.dot(normed, out_w[...], preferred_element_type=F32)
    for j in range(width // 128):
        held[j] = mix[:, 128 * j : 128 * j + 128]
    for k in range(width // 256):
        keep_ref[k] = held[2 * k + core]
        give_ref[k] = held[2 * k + 1 - core].astype(BF)
    back.wait()


def pair_kernel(keep_ref, got_ref, sent_ref):
    pair = (keep_ref[...] + got_ref[...].astype(F32)).astype(BF)
    for n in range(sent_ref.shape[0]):
        sent_ref[n] = pair


def dispatch_kernel(pairs_ref, tokens_ref, select_ref, sent_ref, own_ref, held):
    rows = tokens_ref.shape[0]
    blocks = pairs_ref.shape[1]
    core = lax.axis_index("c")
    mine = []
    for k in range(blocks):
        at = pl.multiple_of((2 * k + core) * 128, 128)
        m = tokens_ref[:, pl.ds(at, 128)].astype(F32)
        for p in range(pairs_ref.shape[0]):
            m = m + pairs_ref[p, k].astype(F32)
        held[k] = m
        mine.append(m)
    own_ref[...] = held[lax.axis_index("x")]
    mine = jnp.concatenate(mine, axis=0).astype(BF)
    count, _, wide = select_ref.shape
    same = lax.broadcasted_iota(jnp.int32, (blocks, wide), 0) == (
        lax.broadcasted_iota(jnp.int32, (blocks, wide), 1) // rows
    )
    spread = jnp.broadcast_to(select_ref[...], (count, blocks, wide)) * same.astype(F32)[None]
    spread = spread.reshape(count * blocks, wide).astype(BF)
    sent_ref[...] = jnp.dot(spread, mine, preferred_element_type=F32).astype(BF)


def columns(ref, parity, blocks):
    return jnp.concatenate(
        [ref[:, pl.ds(pl.multiple_of((2 * k + parity) * 128, 128), 128)] for k in range(blocks)],
        axis=1,
    )


def gains(ref, k, parity):
    return ref[pl.ds(2 * k + parity, 1), :]


def project(x_ref, parity, gain_ref, bias_ref, gate_ref, up_ref, dense_ref):
    count, half_width = x_ref.shape
    blocks = half_width // 128
    half = dense_ref.shape[1] // 3
    half = half - half % 4
    square = jnp.zeros((count, 128), F32)
    along = jnp.zeros((count, 128), F32)
    parts = []
    for k in range(blocks):
        x = x_ref[:, 128 * k : 128 * k + 128].astype(F32)
        square = square + x * x
        x = x * gains(gain_ref, k, parity)
        along = along + x * gains(bias_ref, k, parity)
        parts.append(x.astype(BF))
    x = jnp.concatenate(parts, axis=1)
    dense = jnp.concatenate(
        [dense_ref[2 * k + parity, : 2 * half, :] for k in range(blocks)], axis=1
    )
    sums = [
        lax.dot_general(x, w, NT, preferred_element_type=F32)
        for w in (columns(gate_ref, parity, blocks), columns(up_ref, parity, blocks), dense)
    ]
    return (*sums, square, along)


def first_kernel(
    x_ref, gain_ref, bias_ref, gate_ref, up_ref, dense_ref, g_ref, u_ref, d_ref, s_ref, a_ref
):
    core = lax.axis_index("c")
    results = project(x_ref, core, gain_ref, bias_ref, gate_ref, up_ref, dense_ref)
    for ref, value in zip((g_ref, u_ref, d_ref, s_ref, a_ref), results):
        ref[...] = value


def expand(hidden, dense_hidden, branch, parity, down_ref, dense_ref, blocks):
    half = dense_hidden.shape[1]
    down = jnp.concatenate(
        [dense_ref[2 * k + parity, 2 * half : 3 * half, :] for k in range(blocks)], axis=1
    )
    r = jnp.dot(hidden, columns(down_ref, parity, blocks), preferred_element_type=F32)
    return r + branch * jnp.dot(dense_hidden, down, preferred_element_type=F32)


def second_kernel(
    x_ref,
    gain_ref,
    bias_ref,
    gate_ref,
    up_ref,
    dense_ref,
    down_ref,
    g_ref,
    u_ref,
    d_ref,
    s_ref,
    a_ref,
    give_ref,
    hidden_ref,
    dense_hidden_ref,
    branch_ref,
):
    count, half_width = x_ref.shape
    other = 1 - lax.axis_index("c")
    results = project(x_ref, other, gain_ref, bias_ref, gate_ref, up_ref, dense_ref)
    gate, up, dense, square, along = [
        ref[...] + value for ref, value in zip((g_ref, u_ref, d_ref, s_ref, a_ref), results)
    ]
    half = dense.shape[1] // 2
    scale = lax.rsqrt(jnp.sum(square, axis=1, keepdims=True) / (2 * half_width) + RMS_EPSILON)
    branch = jax.nn.sigmoid(jnp.sum(along, axis=1, keepdims=True) * scale)
    is_dense = lax.broadcasted_iota(jnp.int32, (count, 1), 0) % 3 == 2

    def gated(v, w):
        v = v * scale
        return (v / (1.0 + jnp.exp(-v))) * (w * scale)

    hidden = jnp.where(is_dense, 0.0, gated(gate, up)).astype(BF)
    dense_hidden = jnp.where(is_dense, gated(dense[:, :half], dense[:, half:]), 0.0).astype(BF)
    r = expand(hidden, dense_hidden, branch, other, down_ref, dense_ref, half_width // 128)
    give_ref[...] = r.astype(BF)
    hidden_ref[...] = hidden
    dense_hidden_ref[...] = dense_hidden
    branch_ref[...] = jnp.broadcast_to(branch, branch_ref.shape)


def third_kernel(hidden_ref, dense_hidden_ref, branch_ref, down_ref, dense_ref, keep_ref):
    keep_ref[...] = expand(
        hidden_ref[...],
        dense_hidden_ref[...],
        branch_ref[:, :1],
        lax.axis_index("c"),
        down_ref,
        dense_ref,
        keep_ref.shape[1] // 128,
    )


def combine_kernel(weight_ref, back_ref, out_ref):
    rows, count = weight_ref.shape
    row = lax.broadcasted_iota(jnp.int32, (rows, count), 0)
    place = lax.broadcasted_iota(jnp.int32, (rows, count), 1)
    dense = (row == lax.axis_index("x")) & (place % 3 == 2)
    weight = jnp.where(dense, 1.0, weight_ref[...])
    high = weight.astype(BF)
    low = (weight - high.astype(F32)).astype(BF)
    back = back_ref[...]
    total = jnp.dot(high, back, preferred_element_type=F32) + jnp.dot(
        low, back, preferred_element_type=F32
    )
    for k in range(out_ref.shape[0]):
        out_ref[k] = total[:, 128 * k : 128 * k + 128]


def swap(x):
    return lax.ppermute(x, "c", [(0, 1), (1, 0)])


def local(
    tokens,
    past_lengths,
    state,
    norm1_gain,
    query_weight,
    key_weight,
    value_weight,
    out_weight,
    norm2_gain,
    branch_gate,
    route_ids,
    route_weights,
    expert_gate,
    expert_up,
    expert_down,
    dense_gate,
    dense_up,
    dense_down,
):
    rows, width = tokens.shape
    x_count = lax.axis_size("x")
    tp_count = 2 * x_count
    ep_count = lax.axis_size(EP)
    x_index = lax.axis_index("x")
    tp_index = lax.axis_index(TP)
    blocks = width // 128
    own_blocks = blocks // 2
    key_size = query_weight.shape[1]
    value_size = value_weight.shape[1]
    smem = pl.BlockSpec(memory_space=pltpu.SMEM)
    vmem = pl.BlockSpec(memory_space=pltpu.VMEM)
    hbm = pl.BlockSpec(memory_space=pltpu.HBM)
    shaped = jax.ShapeDtypeStruct

    half = dense_gate.shape[1] // 2
    packed = -(-3 * half // 8) * 8
    sent = call(
        regroup_kernel,
        shaped((x_count, 2, packed, 128), BF),
        (dense_gate.T, dense_up.T, dense_down),
        1_000_000,
        scratch=(
            pltpu.VMEM((3, *dense_down.shape), BF),
            pltpu.VMEM((2, packed, 128), BF),
            pltpu.SemaphoreType.DMA((x_count + 3,)),
        ),
        specs=[hbm, hbm, hbm],
        out_specs=hbm,
        vmem=FULL,
    )
    dense_parts = lax.all_to_all(
        sent.reshape(tp_count, packed, 128), TP, 0, 0, tiled=True
    )

    lane = jnp.arange(key_size, dtype=jnp.int32)
    inverse = 10000.0 ** (-(lane % (key_size // 2)).astype(F32) / (key_size // 2))
    angles = past_lengths.astype(F32)[:, None] * inverse[None, :]
    cosine = jnp.cos(angles)
    sine = jnp.sin(angles) * jnp.where(lane < key_size // 2, -1.0, 1.0)[None, :]
    decay = jnp.exp(jnp.log1p(-jnp.exp2(-5.0 - 7.0 * tp_index.astype(F32) / (tp_count - 1))))
    keep, give, new_state = call(
        retention_kernel,
        (
            shaped((own_blocks, rows, 128), F32),
            shaped((own_blocks, rows, 128), BF),
            shaped((rows, key_size, value_size), F32),
        ),
        (
            tokens,
            norm1_gain.reshape(1, width),
            cosine,
            sine,
            decay.reshape(1),
            query_weight,
            key_weight,
            value_weight,
            state.reshape(rows, key_size, value_size),
            out_weight,
        ),
        10_000_000_000,
        scratch=(
            pltpu.VMEM(query_weight.shape, BF),
            pltpu.VMEM(key_weight.shape, BF),
            pltpu.VMEM(value_weight.shape, BF),
            pltpu.VMEM((rows, key_size, value_size), F32),
            pltpu.VMEM(out_weight.shape, BF),
            pltpu.VMEM((rows, key_size, value_size), F32),
            pltpu.VMEM((blocks, rows, 128), F32),
            pltpu.SemaphoreType.DMA((6,)),
        ),
        specs=[vmem, vmem, vmem, vmem, smem, hbm, hbm, hbm, hbm, hbm],
        out_specs=(vmem, vmem, hbm),
        vmem=FULL,
    )
    route_count = route_ids.shape[1]
    route_flat = route_ids.reshape(-1)
    same = (route_flat[:, None] == route_flat[None, :]).astype(jnp.int32)
    number = jnp.arange(rows * route_count, dtype=jnp.int32)
    slot_index = jnp.sum(same * (number[None, :] < number[:, None]), axis=1)
    place_of = jnp.where(slot_index < 2, route_flat * 3 + slot_index, -1)
    place_of = place_of.reshape(rows, route_count)
    in_row = jnp.arange(3 * ep_count, dtype=jnp.int32)
    row_kind = (in_row // 12) * 3 + in_row % 3
    weighted = jnp.sum(
        jnp.where(place_of[:, :, None] == row_kind, route_weights[:, :, None], 0.0), axis=1
    )
    token = jnp.arange(own_blocks * rows, dtype=jnp.int32) % rows
    tiled = jnp.tile(place_of, (own_blocks, 1))
    chosen = jnp.any(tiled[None] == row_kind[:, None, None], axis=2) | (
        (in_row[:, None] % 3 == 2) & (token[None, :] == x_index)
    )
    select = chosen.astype(F32)[:, None, :]

    sent = call(
        pair_kernel,
        shaped((x_count, own_blocks, rows, 128), BF),
        (keep, swap(give)),
        1_000_000,
    )
    sent, select, weighted = lax.optimization_barrier((sent, select, weighted))
    pairs = lax.all_to_all(sent, "x", 0, 0, tiled=True)

    outgoing, own = call(
        dispatch_kernel,
        (shaped((3 * ep_count * own_blocks, 128), BF), shaped((rows, 128), F32)),
        (pairs, tokens, select),
        1_000_000_000,
        scratch=(pltpu.VMEM((own_blocks, rows, 128), F32),),
    )
    arrived = lax.all_to_all(outgoing.reshape(ep_count, 3 * own_blocks, 128), EP, 0, 0, tiled=True)
    count = 3 * ep_count
    shape = (count, width // 2)
    weights = (
        norm2_gain.reshape(blocks, 128),
        branch_gate.reshape(blocks, 128),
        expert_gate[0].T,
        expert_up[0].T,
        dense_parts,
    )
    down = expert_down[0]
    mine = arrived.reshape(shape)
    other = swap(mine)
    partials = call(
        first_kernel,
        tuple(shaped((count, n), F32) for n in (down.shape[0], down.shape[0], 2 * half, 128, 128)),
        (mine, *weights),
        2_000_000_000,
    )
    leave, hidden, dense_hidden, branch = call(
        second_kernel,
        (
            shaped(shape, BF),
            shaped((count, down.shape[0]), BF),
            shaped((count, half), BF),
            shaped((count, 128), F32),
        ),
        (other, *weights, down, *partials),
        2_000_000_000,
    )
    stay = call(
        third_kernel,
        shaped(shape, F32),
        (hidden, dense_hidden, branch, down, dense_parts),
        2_000_000_000,
    )
    result = (stay + swap(leave).astype(F32)).astype(BF)
    returned = lax.all_to_all(result.reshape(ep_count, 3 * own_blocks, 128), EP, 0, 0, tiled=True)
    total = call(
        combine_kernel,
        shaped((own_blocks, rows, 128), F32),
        (weighted, returned.reshape(shape)),
        100_000_000,
    )
    sums = lax.all_to_all(total, "x", 0, 0, tiled=True)
    layer_out = (own + jnp.sum(sums, axis=0)).astype(BF)
    return (layer_out, new_state.reshape(state.shape))


def solution(mesh):
    split = Mesh(mesh.devices.reshape(8, 8, 8, 2), ("z", "y", "x", "c"))
    return jax.shard_map(
        local,
        mesh=split,
        in_specs=(
            P(EP, None),
            P(EP),
            P(EP, TP, None, None),
            P(),
            P(None, TP),
            P(None, TP),
            P(None, TP),
            P(TP, None),
            P(),
            P(),
            P(EP, None),
            P(EP, None),
            P(EP, None, TP),
            P(EP, None, TP),
            P(EP, TP, None),
            P(TP, EP),
            P(TP, EP),
            P(EP, TP),
        ),
        out_specs=(P(EP, TP), P(EP, TP, None, None)),
        check_vma=False,
    )
```

```python
import jax
import jax.numpy as jnp
from jax import lax
from jax.experimental import pallas as pl
from jax.experimental.pallas import tpu as pltpu
from jax.sharding import Mesh
from jax.sharding import PartitionSpec as P

RMS_EPSILON = 1e-06
GROUP_EPSILON = 1e-05
BF = jnp.bfloat16
F32 = jnp.float32
EP = ("z", "y")
TP = ("x", "c")
NT = (((1,), (1,)), ((), ()))
FULL = 58 << 20


def call(kernel, out_shape, args, flops, scratch=(), specs=None, out_specs=None, vmem=None):
    full = pl.BlockSpec(memory_space=pltpu.VMEM)
    size = sum(a.size * a.dtype.itemsize for a in args)
    return pl.pallas_call(
        kernel,
        out_shape=out_shape,
        in_specs=specs or [full] * len(args),
        out_specs=out_specs or jax.tree.map(lambda _: full, out_shape),
        scratch_shapes=list(scratch),
        compiler_params=pltpu.CompilerParams(vmem_limit_bytes=vmem or 16 << 20),
        cost_estimate=pl.CostEstimate(flops=flops, bytes_accessed=size, transcendentals=0),
    )(*args)


def regroup_kernel(gate_hbm, up_hbm, down_hbm, sent_hbm, packed, sems):
    size = gate_hbm.shape[0]
    count = sent_hbm.shape[0]
    copies = [
        pltpu.make_async_copy(ref, packed.at[pl.ds(size * n, size)], sems.at[count + n])
        for n, ref in enumerate((gate_hbm, up_hbm, down_hbm))
    ]
    for c in copies:
        c.start()
    for c in copies:
        c.wait()
    copies = [pltpu.make_async_copy(packed, sent_hbm.at[n], sems.at[n]) for n in range(count)]
    for c in copies:
        c.start()
    for c in copies:
        c.wait()


def trade_kernel(gate_hbm, up_hbm, down_hbm, out_ref, sems):
    size, width = down_hbm.shape
    blocks = width // 256
    other = 1 - lax.axis_index("c")
    copies = []
    for n, ref in enumerate((gate_hbm, up_hbm)):
        for k in range(blocks):
            at = pl.ds(pl.multiple_of((2 * k + other) * 128, 128), 128)
            copies.append((ref.at[:, at], (n, pl.ds(128 * k, 128))))
    for n in range(2):
        copies.append((down_hbm.at[:, pl.ds(n * width // 2, width // 2)], (2 + n, slice(None))))
    copies = [
        pltpu.make_async_copy(src, out_ref.at[pl.ds(size * n, size), lanes], sems.at[i])
        for i, (src, (n, lanes)) in enumerate(copies)
    ]
    for c in copies:
        c.start()
    for c in copies:
        c.wait()


def retention_kernel(
    tokens_ref,
    gain_ref,
    cos_ref,
    sin_ref,
    decay_ref,
    q_hbm,
    k_hbm,
    v_hbm,
    state_hbm,
    out_hbm,
    keep_ref,
    give_ref,
    new_hbm,
    q_w,
    k_w,
    v_w,
    state,
    out_w,
    fresh,
    held,
    sems,
):
    rows, width = tokens_ref.shape
    core = lax.axis_index("c")
    copies = [
        pltpu.make_async_copy(s, d, sems.at[n])
        for n, (s, d) in enumerate(
            ((q_hbm, q_w), (k_hbm, k_w), (v_hbm, v_w), (state_hbm, state), (out_hbm, out_w))
        )
    ]
    for c in copies:
        c.start()
    x = tokens_ref[...].astype(F32)
    inv = lax.rsqrt(jnp.sum(x * x, axis=1, keepdims=True) / width + RMS_EPSILON)
    normed_in = (x * inv * gain_ref[...]).astype(BF)

    def project(n, w):
        copies[n].wait()
        return jnp.dot(normed_in, w[...], preferred_element_type=F32)

    def rotated(v):
        return v * cos_ref[...] + pltpu.roll(v, v.shape[1] // 2, 1) * sin_ref[...]

    query = rotated(project(0, q_w))
    keys = rotated(project(1, k_w)) * q_w.shape[1] ** (-0.5)
    values = project(2, v_w)
    query_t = query.T
    keys_t = keys.T
    copies[3].wait()
    decay = decay_ref[0]
    retained = []
    for i in range(rows):
        new = state[i] * decay + keys_t[:, i : i + 1] * values[i : i + 1, :]
        fresh[i] = new
        retained.append(jnp.sum(query_t[:, i : i + 1] * new, axis=0, keepdims=True))
    back = pltpu.make_async_copy(fresh, new_hbm, sems.at[5])
    back.start()
    retained = jnp.concatenate(retained, axis=0)
    centered = retained - jnp.mean(retained, axis=1, keepdims=True)
    normed = centered * lax.rsqrt(
        jnp.mean(centered * centered, axis=1, keepdims=True) + GROUP_EPSILON
    )
    normed = normed.astype(BF)
    copies[4].wait()
    mix = jnp.dot(normed, out_w[...], preferred_element_type=F32)
    for j in range(width // 128):
        held[j] = mix[:, 128 * j : 128 * j + 128]
    for k in range(width // 256):
        keep_ref[k] = held[2 * k + core]
        give_ref[k] = held[2 * k + 1 - core].astype(BF)
    back.wait()


def pair_kernel(keep_ref, got_ref, sent_ref):
    pair = (keep_ref[...] + got_ref[...].astype(F32)).astype(BF)
    for n in range(sent_ref.shape[0]):
        sent_ref[n] = pair


def dispatch_kernel(pairs_ref, tokens_ref, select_ref, sent_ref, own_ref, held):
    rows = tokens_ref.shape[0]
    blocks = pairs_ref.shape[1]
    core = lax.axis_index("c")
    mine = []
    for k in range(blocks):
        at = pl.multiple_of((2 * k + core) * 128, 128)
        m = tokens_ref[:, pl.ds(at, 128)].astype(F32)
        for p in range(pairs_ref.shape[0]):
            m = m + pairs_ref[p, k].astype(F32)
        held[k] = m
        mine.append(m)
    own_ref[...] = held[lax.axis_index("x")]
    mine = jnp.concatenate(mine, axis=0).astype(BF)
    count, _, wide = select_ref.shape
    same = lax.broadcasted_iota(jnp.int32, (blocks, wide), 0) == (
        lax.broadcasted_iota(jnp.int32, (blocks, wide), 1) // rows
    )
    spread = jnp.broadcast_to(select_ref[...], (count, blocks, wide)) * same.astype(F32)[None]
    spread = spread.reshape(count * blocks, wide).astype(BF)
    sent_ref[...] = jnp.dot(spread, mine, preferred_element_type=F32).astype(BF)


def columns(ref, parity, blocks):
    return jnp.concatenate(
        [ref[:, pl.ds(pl.multiple_of((2 * k + parity) * 128, 128), 128)] for k in range(blocks)],
        axis=1,
    )


def gains(ref, k, parity):
    return ref[pl.ds(2 * k + parity, 1), :]


def first_kernel(
    x_ref, gain_ref, bias_ref, gate_ref, up_ref, got_ref, dense_ref, keep_ref, give_ref, sums
):
    count, half_width = x_ref.shape
    third = count // 3
    blocks = half_width // 128
    wide = gate_ref.shape[0]
    size = dense_ref.shape[1] // 3
    core = lax.axis_index("c")
    square = jnp.zeros((count, 128), F32)
    along = jnp.zeros((third, 128), F32)
    parts = []
    for k in range(blocks):
        x = x_ref[:, 128 * k : 128 * k + 128].astype(F32)
        square = square + x * x
        x = x * gains(gain_ref, k, core)
        along = along + x[2 * third :] * gains(bias_ref, k, core)
        parts.append(x.astype(BF))
    x = jnp.concatenate(parts, axis=1)

    def apply(rows, w):
        return lax.dot_general(rows, w, NT, preferred_element_type=F32)

    rows = x[: 2 * third]
    sums[:, :] = jnp.zeros(sums.shape, F32)
    sums[:, 0:wide] = apply(rows, columns(gate_ref, core, blocks))
    sums[:, 128 : 128 + wide] = apply(rows, got_ref[:wide, :])
    sums[:, 256 : 256 + wide] = apply(rows, columns(up_ref, core, blocks))
    sums[:, 384 : 384 + wide] = apply(rows, got_ref[wide : 2 * wide, :])
    sums[:, 512:640] = jnp.broadcast_to(
        jnp.sum(square[: 2 * third], axis=1, keepdims=True), (2 * third, 128)
    )
    own = pl.ds(pl.multiple_of(core * third, third), third)
    other = pl.ds(pl.multiple_of((1 - core) * third, third), third)
    keep_ref[:, :512] = sums[own, :512]
    for p, q in enumerate((1, 0, 3, 2)):
        give_ref[:, 128 * p : 128 * p + 128] = sums[other, 128 * q : 128 * q + 128]
    rows = x[2 * third :]
    lane = lax.broadcasted_iota(jnp.int32, (third, 128), 1)
    both = jnp.where(
        lane < 64,
        jnp.sum(square[2 * third :], axis=1, keepdims=True),
        jnp.sum(along, axis=1, keepdims=True),
    )
    for ref, at in ((keep_ref, own), (give_ref, other)):
        ref[:, 768:896] = jnp.where(lane < 32, sums[at, 512:640], both)
    for n in range(2):
        w = jnp.concatenate(
            [dense_ref[k, size * n : size * n + size, :] for k in range(blocks)], axis=1
        )
        part = jnp.concatenate(
            [apply(rows, w), jnp.zeros((third, 128 - size), F32)], axis=1
        )
        keep_ref[:, 512 + 128 * n : 640 + 128 * n] = part
        give_ref[:, 512 + 128 * n : 640 + 128 * n] = part


def second_kernel(keep_ref, got_ref, down_ref, traded_ref, dense_ref, out_ref):
    wide, width = down_ref.shape
    blocks, size = dense_ref.shape[0], dense_ref.shape[1] // 3
    stats = keep_ref[:, 768:896] + got_ref[:, 768:896]

    def scale(value):
        return lax.rsqrt(value / width + RMS_EPSILON)

    def gated(at, to, count, factor):
        v = (keep_ref[:, at : at + count] + got_ref[:, at : at + count]) * factor
        w = (keep_ref[:, to : to + count] + got_ref[:, to : to + count]) * factor
        return ((v / (1.0 + jnp.exp(-v))) * w).astype(BF)

    factor = scale(stats[:, 0:1])
    own = gated(0, 256, wide, factor)
    other = gated(128, 384, wide, factor)
    for n in range(2):
        at = slice(n * width // 2, (n + 1) * width // 2)
        r = jnp.dot(own, down_ref[:, at], preferred_element_type=F32)
        r = r + jnp.dot(
            other, traded_ref[(2 + n) * wide : (3 + n) * wide, :], preferred_element_type=F32
        )
        out_ref[:, at] = r.astype(BF)
    factor = scale(stats[:, 32:33])
    branch = jax.nn.sigmoid(stats[:, 64:65] * factor)
    hidden = gated(512, 640, size, factor)
    w = jnp.concatenate([dense_ref[k, 2 * size :, :] for k in range(blocks)], axis=1)
    r = branch * jnp.dot(hidden, w, preferred_element_type=F32)
    out_ref[:, width:] = r.astype(BF)


def combine_kernel(weight_ref, back_ref, out_ref):
    rows = weight_ref.shape[0]
    blocks = out_ref.shape[0]
    width = 128 * blocks
    core = lax.axis_index("c")
    weight = weight_ref[...]
    high = weight.astype(BF)
    low = (weight - high.astype(F32)).astype(BF)
    back = back_ref[:, :width]
    total = jnp.dot(high, back, preferred_element_type=F32) + jnp.dot(
        low, back, preferred_element_type=F32
    )
    for j in range(blocks):
        out_ref[j] = total[:, 128 * j : 128 * j + 128]
    here = lax.broadcasted_iota(jnp.int32, (rows, 128), 0) == lax.axis_index("x")
    for k in range(blocks // 2):
        dense = back_ref[:, width + 128 * k : width + 128 * k + 128].astype(F32)
        dense = jnp.sum(dense, axis=0, keepdims=True)
        out_ref[2 * k + core] = out_ref[2 * k + core] + jnp.where(here, dense, 0.0)


def swap(x):
    return lax.ppermute(x, "c", [(0, 1), (1, 0)])


def local(
    tokens,
    past_lengths,
    state,
    norm1_gain,
    query_weight,
    key_weight,
    value_weight,
    out_weight,
    norm2_gain,
    branch_gate,
    route_ids,
    route_weights,
    expert_gate,
    expert_up,
    expert_down,
    dense_gate,
    dense_up,
    dense_down,
):
    rows, width = tokens.shape
    x_count = lax.axis_size("x")
    tp_count = 2 * x_count
    ep_count = lax.axis_size(EP)
    x_index = lax.axis_index("x")
    tp_index = lax.axis_index(TP)
    blocks = width // 128
    own_blocks = blocks // 2
    key_size = query_weight.shape[1]
    value_size = value_weight.shape[1]
    smem = pl.BlockSpec(memory_space=pltpu.SMEM)
    vmem = pl.BlockSpec(memory_space=pltpu.VMEM)
    hbm = pl.BlockSpec(memory_space=pltpu.HBM)
    shaped = jax.ShapeDtypeStruct

    size = dense_down.shape[0]
    sent = call(
        regroup_kernel,
        shaped((x_count, 3 * size, 128), BF),
        (dense_gate.T, dense_up.T, dense_down),
        1_000_000,
        scratch=(
            pltpu.VMEM((3 * size, 128), BF),
            pltpu.SemaphoreType.DMA((x_count + 3,)),
        ),
        specs=[hbm, hbm, hbm],
        out_specs=hbm,
        vmem=FULL,
    )
    dense_parts = lax.all_to_all(sent, "x", 0, 0, tiled=True)

    gate_rows, up_rows, down = expert_gate[0].T, expert_up[0].T, expert_down[0]
    traded = swap(
        call(
            trade_kernel,
            shaped((4 * down.shape[0], width // 2), BF),
            (gate_rows, up_rows, down),
            1_000_000,
            scratch=(pltpu.SemaphoreType.DMA((blocks + 2,)),),
            specs=[hbm, hbm, hbm],
            vmem=FULL,
        )
    )

    lane = jnp.arange(key_size, dtype=jnp.int32)
    inverse = 10000.0 ** (-(lane % (key_size // 2)).astype(F32) / (key_size // 2))
    angles = past_lengths.astype(F32)[:, None] * inverse[None, :]
    cosine = jnp.cos(angles)
    sine = jnp.sin(angles) * jnp.where(lane < key_size // 2, -1.0, 1.0)[None, :]
    decay = jnp.exp(jnp.log1p(-jnp.exp2(-5.0 - 7.0 * tp_index.astype(F32) / (tp_count - 1))))
    keep, give, new_state = call(
        retention_kernel,
        (
            shaped((own_blocks, rows, 128), F32),
            shaped((own_blocks, rows, 128), BF),
            shaped((rows, key_size, value_size), F32),
        ),
        (
            tokens,
            norm1_gain.reshape(1, width),
            cosine,
            sine,
            decay.reshape(1),
            query_weight,
            key_weight,
            value_weight,
            state.reshape(rows, key_size, value_size),
            out_weight,
        ),
        10_000_000_000,
        scratch=(
            pltpu.VMEM(query_weight.shape, BF),
            pltpu.VMEM(key_weight.shape, BF),
            pltpu.VMEM(value_weight.shape, BF),
            pltpu.VMEM((rows, key_size, value_size), F32),
            pltpu.VMEM(out_weight.shape, BF),
            pltpu.VMEM((rows, key_size, value_size), F32),
            pltpu.VMEM((blocks, rows, 128), F32),
            pltpu.SemaphoreType.DMA((6,)),
        ),
        specs=[vmem, vmem, vmem, vmem, smem, hbm, hbm, hbm, hbm, hbm],
        out_specs=(vmem, vmem, hbm),
        vmem=FULL,
    )
    route_count = route_ids.shape[1]
    route_flat = route_ids.reshape(-1)
    same = (route_flat[:, None] == route_flat[None, :]).astype(jnp.int32)
    number = jnp.arange(rows * route_count, dtype=jnp.int32)
    slot_index = jnp.sum(same * (number[None, :] < number[:, None]), axis=1)
    place_of = jnp.where(slot_index < 2, route_flat * 3 + slot_index, -1)
    place_of = place_of.reshape(rows, route_count)
    in_row = jnp.arange(3 * ep_count, dtype=jnp.int32)
    row_kind = (in_row // 12) * 3 + in_row % 3
    slot_kind = (jnp.arange(ep_count, dtype=jnp.int32) // 4) * 3 + lax.axis_index("c")
    weighted = jnp.sum(
        jnp.where(place_of[:, :, None] == slot_kind, route_weights[:, :, None], 0.0), axis=1
    )
    token = jnp.arange(own_blocks * rows, dtype=jnp.int32) % rows
    tiled = jnp.tile(place_of, (own_blocks, 1))
    chosen = jnp.any(tiled[None] == row_kind[:, None, None], axis=2) | (
        (in_row[:, None] % 3 == 2) & (token[None, :] == x_index)
    )
    select = chosen.astype(F32)[:, None, :]

    sent = call(
        pair_kernel,
        shaped((x_count, own_blocks, rows, 128), BF),
        (keep, swap(give)),
        1_000_000,
    )
    sent, select, weighted = lax.optimization_barrier((sent, select, weighted))
    pairs = lax.all_to_all(sent, "x", 0, 0, tiled=True)

    outgoing, own = call(
        dispatch_kernel,
        (shaped((3 * ep_count * own_blocks, 128), BF), shaped((rows, 128), F32)),
        (pairs, tokens, select),
        1_000_000_000,
        scratch=(pltpu.VMEM((own_blocks, rows, 128), F32),),
    )
    arrived = lax.all_to_all(outgoing.reshape(ep_count, 3 * own_blocks, 128), EP, 0, 0, tiled=True)
    mine = arrived.reshape(ep_count, 3, own_blocks, 128).transpose(1, 0, 2, 3)
    mine = mine.reshape(3 * ep_count, width // 2)
    message = shaped((ep_count, 7 * 128), F32)
    kept, given = call(
        first_kernel,
        (message, message),
        (
            mine,
            norm2_gain.reshape(blocks, 128),
            branch_gate.reshape(blocks, 128),
            gate_rows,
            up_rows,
            traded,
            dense_parts,
        ),
        2_000_000_000,
        scratch=(pltpu.VMEM((2 * ep_count, 640), F32),),
    )
    result = call(
        second_kernel,
        shaped((ep_count, 3 * width // 2), BF),
        (kept, swap(given), down, traded, dense_parts),
        2_000_000_000,
    )
    returned = lax.all_to_all(result.reshape(ep_count, 3 * own_blocks, 128), EP, 0, 0, tiled=True)
    total = call(
        combine_kernel,
        shaped((blocks, rows, 128), F32),
        (weighted, returned.reshape(ep_count, 3 * width // 2)),
        100_000_000,
    )
    sums = lax.all_to_all(total, TP, 0, 0, tiled=True)
    layer_out = (own + jnp.sum(sums, axis=0)).astype(BF)
    return (layer_out, new_state.reshape(state.shape))


def solution(mesh):
    split = Mesh(mesh.devices.reshape(8, 8, 8, 2), ("z", "y", "x", "c"))
    return jax.shard_map(
        local,
        mesh=split,
        in_specs=(
            P(EP, None),
            P(EP),
            P(EP, TP, None, None),
            P(),
            P(None, TP),
            P(None, TP),
            P(None, TP),
            P(TP, None),
            P(),
            P(),
            P(EP, None),
            P(EP, None),
            P(EP, None, TP),
            P(EP, None, TP),
            P(EP, TP, None),
            P(TP, EP),
            P(TP, EP),
            P(EP, TP),
        ),
        out_specs=(P(EP, TP), P(EP, TP, None, None)),
        check_vma=False,
    )
```

```python
import jax
import jax.numpy as jnp
from jax import lax
from jax.experimental import pallas as pl
from jax.experimental.pallas import tpu as pltpu
from jax.sharding import Mesh
from jax.sharding import PartitionSpec as P

RMS_EPSILON = 1e-06
GROUP_EPSILON = 1e-05
BF = jnp.bfloat16
F32 = jnp.float32
EP = ("z", "y")
TP = ("x", "c")
NT = (((1,), (1,)), ((), ()))
FULL = 58 << 20
TRADE = 16 << 20


def call(kernel, out_shape, args, flops, scratch=(), specs=None, out_specs=None, vmem=None):
    full = pl.BlockSpec(memory_space=pltpu.VMEM)
    size = sum(a.size * a.dtype.itemsize for a in args)
    return pl.pallas_call(
        kernel,
        out_shape=out_shape,
        in_specs=specs or [full] * len(args),
        out_specs=out_specs or jax.tree.map(lambda _: full, out_shape),
        scratch_shapes=list(scratch),
        compiler_params=pltpu.CompilerParams(vmem_limit_bytes=vmem or 16 << 20),
        cost_estimate=pl.CostEstimate(flops=flops, bytes_accessed=size, transcendentals=0),
    )(*args)


def regroup_kernel(gate_hbm, up_hbm, down_hbm, sent_hbm, packed, sems):
    size = gate_hbm.shape[0]
    count = sent_hbm.shape[0]
    copies = [
        pltpu.make_async_copy(ref, packed.at[pl.ds(size * n, size)], sems.at[count + n])
        for n, ref in enumerate((gate_hbm, up_hbm, down_hbm))
    ]
    for c in copies:
        c.start()
    for c in copies:
        c.wait()
    copies = [pltpu.make_async_copy(packed, sent_hbm.at[n], sems.at[n]) for n in range(count)]
    for c in copies:
        c.start()
    for c in copies:
        c.wait()


def trade_kernel(gate_hbm, up_hbm, down_hbm, out_ref, sems):
    size, width = down_hbm.shape
    blocks = width // 256
    other = 1 - lax.axis_index("c")
    copies = []
    for n, ref in enumerate((gate_hbm, up_hbm)):
        for k in range(blocks):
            at = pl.ds(pl.multiple_of((2 * k + other) * 128, 128), 128)
            copies.append((ref.at[:, at], (n, pl.ds(128 * k, 128))))
    for n in range(2):
        copies.append((down_hbm.at[:, pl.ds(n * width // 2, width // 2)], (2 + n, slice(None))))
    copies = [
        pltpu.make_async_copy(src, out_ref.at[pl.ds(size * n, size), lanes], sems.at[i])
        for i, (src, (n, lanes)) in enumerate(copies)
    ]
    for c in copies:
        c.start()
    for c in copies:
        c.wait()


def retention_kernel(
    tokens_ref,
    gain_ref,
    cos_ref,
    sin_ref,
    decay_ref,
    q_hbm,
    k_hbm,
    v_hbm,
    state_hbm,
    out_hbm,
    keep_ref,
    give_ref,
    new_hbm,
    q_w,
    k_w,
    v_w,
    state,
    out_w,
    fresh,
    held,
    sems,
):
    rows, width = tokens_ref.shape
    core = lax.axis_index("c")
    copies = [
        pltpu.make_async_copy(s, d, sems.at[n])
        for n, (s, d) in enumerate(
            ((q_hbm, q_w), (k_hbm, k_w), (v_hbm, v_w), (state_hbm, state), (out_hbm, out_w))
        )
    ]
    for c in copies:
        c.start()
    x = tokens_ref[...].astype(F32)
    inv = lax.rsqrt(jnp.sum(x * x, axis=1, keepdims=True) / width + RMS_EPSILON)
    normed_in = (x * inv * gain_ref[...]).astype(BF)

    def project(n, w):
        copies[n].wait()
        return jnp.dot(normed_in, w[...], preferred_element_type=F32)

    def rotated(v):
        return v * cos_ref[...] + pltpu.roll(v, v.shape[1] // 2, 1) * sin_ref[...]

    query = rotated(project(0, q_w))
    keys = rotated(project(1, k_w)) * q_w.shape[1] ** (-0.5)
    values = project(2, v_w)
    query_t = query.T
    keys_t = keys.T
    copies[3].wait()
    decay = decay_ref[0]
    retained = []
    for i in range(rows):
        new = state[i] * decay + keys_t[:, i : i + 1] * values[i : i + 1, :]
        fresh[i] = new
        retained.append(jnp.sum(query_t[:, i : i + 1] * new, axis=0, keepdims=True))
    back = pltpu.make_async_copy(fresh, new_hbm, sems.at[5])
    back.start()
    retained = jnp.concatenate(retained, axis=0)
    centered = retained - jnp.mean(retained, axis=1, keepdims=True)
    normed = centered * lax.rsqrt(
        jnp.mean(centered * centered, axis=1, keepdims=True) + GROUP_EPSILON
    )
    normed = normed.astype(BF)
    copies[4].wait()
    mix = jnp.dot(normed, out_w[...], preferred_element_type=F32)
    for j in range(width // 128):
        held[j] = mix[:, 128 * j : 128 * j + 128]
    for k in range(width // 256):
        keep_ref[k] = held[2 * k + core]
        give_ref[k] = held[2 * k + 1 - core].astype(BF)
    back.wait()


def pair_kernel(keep_ref, got_ref, sent_ref):
    pair = (keep_ref[...] + got_ref[...].astype(F32)).astype(BF)
    for n in range(sent_ref.shape[0]):
        sent_ref[n] = pair


def dispatch_kernel(pairs_ref, tokens_ref, select_ref, sent_ref, own_ref, held):
    rows = tokens_ref.shape[0]
    blocks = pairs_ref.shape[1]
    core = lax.axis_index("c")
    mine = []
    for k in range(blocks):
        at = pl.multiple_of((2 * k + core) * 128, 128)
        m = tokens_ref[:, pl.ds(at, 128)].astype(F32)
        for p in range(pairs_ref.shape[0]):
            m = m + pairs_ref[p, k].astype(F32)
        held[k] = m
        mine.append(m)
    own_ref[...] = held[lax.axis_index("x")]
    mine = jnp.concatenate(mine, axis=0).astype(BF)
    count, _, wide = select_ref.shape
    same = lax.broadcasted_iota(jnp.int32, (blocks, wide), 0) == (
        lax.broadcasted_iota(jnp.int32, (blocks, wide), 1) // rows
    )
    spread = jnp.broadcast_to(select_ref[...], (count, blocks, wide)) * same.astype(F32)[None]
    spread = spread.reshape(count * blocks, wide).astype(BF)
    sent_ref[...] = jnp.dot(spread, mine, preferred_element_type=F32).astype(BF)


def columns(ref, parity, blocks):
    return jnp.concatenate(
        [ref[:, pl.ds(pl.multiple_of((2 * k + parity) * 128, 128), 128)] for k in range(blocks)],
        axis=1,
    )


def gains(ref, k, parity):
    return ref[pl.ds(2 * k + parity, 1), :]


def first_kernel(
    x_ref,
    gain_ref,
    bias_ref,
    gate_ref,
    up_ref,
    traded_hbm,
    dense_ref,
    keep_ref,
    give_ref,
    sums,
    got_ref,
    sem,
):
    copy = pltpu.make_async_copy(traded_hbm.at[pl.ds(0, got_ref.shape[0])], got_ref, sem)
    copy.start()
    count, half_width = x_ref.shape
    third = count // 3
    blocks = half_width // 128
    wide = gate_ref.shape[0]
    size = dense_ref.shape[1] // 3
    core = lax.axis_index("c")
    square = jnp.zeros((count, 128), F32)
    along = jnp.zeros((third, 128), F32)
    parts = []
    for k in range(blocks):
        x = x_ref[:, 128 * k : 128 * k + 128].astype(F32)
        square = square + x * x
        x = x * gains(gain_ref, k, core)
        along = along + x[2 * third :] * gains(bias_ref, k, core)
        parts.append(x.astype(BF))
    x = jnp.concatenate(parts, axis=1)

    def apply(rows, w):
        return lax.dot_general(rows, w, NT, preferred_element_type=F32)

    rows = x[: 2 * third]
    sums[:, :] = jnp.zeros(sums.shape, F32)
    sums[:, 0:wide] = apply(rows, columns(gate_ref, core, blocks))
    sums[:, 256 : 256 + wide] = apply(rows, columns(up_ref, core, blocks))
    copy.wait()
    sums[:, 128 : 128 + wide] = apply(rows, got_ref[:wide, :])
    sums[:, 384 : 384 + wide] = apply(rows, got_ref[wide : 2 * wide, :])
    sums[:, 512:640] = jnp.broadcast_to(
        jnp.sum(square[: 2 * third], axis=1, keepdims=True), (2 * third, 128)
    )
    own = pl.ds(pl.multiple_of(core * third, third), third)
    other = pl.ds(pl.multiple_of((1 - core) * third, third), third)
    keep_ref[:, :512] = sums[own, :512]
    for p, q in enumerate((1, 0, 3, 2)):
        give_ref[:, 128 * p : 128 * p + 128] = sums[other, 128 * q : 128 * q + 128]
    rows = x[2 * third :]
    lane = lax.broadcasted_iota(jnp.int32, (third, 128), 1)
    both = jnp.where(
        lane < 64,
        jnp.sum(square[2 * third :], axis=1, keepdims=True),
        jnp.sum(along, axis=1, keepdims=True),
    )
    for ref, at in ((keep_ref, own), (give_ref, other)):
        ref[:, 768:896] = jnp.where(lane < 32, sums[at, 512:640], both)
    for n in range(2):
        w = jnp.concatenate(
            [dense_ref[k, size * n : size * n + size, :] for k in range(blocks)], axis=1
        )
        part = jnp.concatenate(
            [apply(rows, w), jnp.zeros((third, 128 - size), F32)], axis=1
        )
        keep_ref[:, 512 + 128 * n : 640 + 128 * n] = part
        give_ref[:, 512 + 128 * n : 640 + 128 * n] = part


def second_kernel(keep_ref, got_ref, down_ref, traded_hbm, dense_ref, out_ref, traded_ref, sem):
    wide, width = down_ref.shape
    copy = pltpu.make_async_copy(traded_hbm.at[pl.ds(2 * wide, 2 * wide)], traded_ref, sem)
    copy.start()
    blocks, size = dense_ref.shape[0], dense_ref.shape[1] // 3
    stats = keep_ref[:, 768:896] + got_ref[:, 768:896]

    def scale(value):
        return lax.rsqrt(value / width + RMS_EPSILON)

    def gated(at, to, count, factor):
        v = (keep_ref[:, at : at + count] + got_ref[:, at : at + count]) * factor
        w = (keep_ref[:, to : to + count] + got_ref[:, to : to + count]) * factor
        return ((v / (1.0 + jnp.exp(-v))) * w).astype(BF)

    factor = scale(stats[:, 32:33])
    branch = jax.nn.sigmoid(stats[:, 64:65] * factor)
    hidden = gated(512, 640, size, factor)
    w = jnp.concatenate([dense_ref[k, 2 * size :, :] for k in range(blocks)], axis=1)
    r = branch * jnp.dot(hidden, w, preferred_element_type=F32)
    out_ref[:, width:] = r.astype(BF)
    factor = scale(stats[:, 0:1])
    own = gated(0, 256, wide, factor)
    other = gated(128, 384, wide, factor)
    copy.wait()
    for n in range(2):
        at = slice(n * width // 2, (n + 1) * width // 2)
        r = jnp.dot(own, down_ref[:, at], preferred_element_type=F32)
        r = r + jnp.dot(
            other, traded_ref[n * wide : (n + 1) * wide, :], preferred_element_type=F32
        )
        out_ref[:, at] = r.astype(BF)


def combine_kernel(weight_ref, back_ref, out_ref):
    rows = weight_ref.shape[0]
    blocks = out_ref.shape[0]
    width = 128 * blocks
    core = lax.axis_index("c")
    weight = weight_ref[...]
    high = weight.astype(BF)
    low = (weight - high.astype(F32)).astype(BF)
    back = back_ref[:, :width]
    total = jnp.dot(high, back, preferred_element_type=F32) + jnp.dot(
        low, back, preferred_element_type=F32
    )
    for j in range(blocks):
        out_ref[j] = total[:, 128 * j : 128 * j + 128]
    here = lax.broadcasted_iota(jnp.int32, (rows, 128), 0) == lax.axis_index("x")
    for k in range(blocks // 2):
        dense = back_ref[:, width + 128 * k : width + 128 * k + 128].astype(F32)
        dense = jnp.sum(dense, axis=0, keepdims=True)
        out_ref[2 * k + core] = out_ref[2 * k + core] + jnp.where(here, dense, 0.0)


def swap(x):
    return lax.ppermute(x, "c", [(0, 1), (1, 0)])


def local(
    tokens,
    past_lengths,
    state,
    norm1_gain,
    query_weight,
    key_weight,
    value_weight,
    out_weight,
    norm2_gain,
    branch_gate,
    route_ids,
    route_weights,
    expert_gate,
    expert_up,
    expert_down,
    dense_gate,
    dense_up,
    dense_down,
):
    rows, width = tokens.shape
    x_count = lax.axis_size("x")
    tp_count = 2 * x_count
    ep_count = lax.axis_size(EP)
    x_index = lax.axis_index("x")
    tp_index = lax.axis_index(TP)
    blocks = width // 128
    own_blocks = blocks // 2
    key_size = query_weight.shape[1]
    value_size = value_weight.shape[1]
    smem = pl.BlockSpec(memory_space=pltpu.SMEM)
    vmem = pl.BlockSpec(memory_space=pltpu.VMEM)
    hbm = pl.BlockSpec(memory_space=pltpu.HBM)
    shaped = jax.ShapeDtypeStruct

    size = dense_down.shape[0]
    sent = call(
        regroup_kernel,
        shaped((x_count, 3 * size, 128), BF),
        (dense_gate.T, dense_up.T, dense_down),
        1_000_000,
        scratch=(
            pltpu.VMEM((3 * size, 128), BF),
            pltpu.SemaphoreType.DMA((x_count + 3,)),
        ),
        specs=[hbm, hbm, hbm],
        out_specs=hbm,
        vmem=FULL,
    )
    dense_parts = lax.all_to_all(sent, "x", 0, 0, tiled=True)

    gate_rows, up_rows, down = expert_gate[0].T, expert_up[0].T, expert_down[0]
    traded = swap(
        call(
            trade_kernel,
            shaped((4 * down.shape[0], width // 2), BF),
            (gate_rows, up_rows, down),
            1_000_000,
            scratch=(pltpu.SemaphoreType.DMA((blocks + 2,)),),
            specs=[hbm, hbm, hbm],
            vmem=TRADE,
        )
    )

    lane = jnp.arange(key_size, dtype=jnp.int32)
    inverse = 10000.0 ** (-(lane % (key_size // 2)).astype(F32) / (key_size // 2))
    angles = past_lengths.astype(F32)[:, None] * inverse[None, :]
    cosine = jnp.cos(angles)
    sine = jnp.sin(angles) * jnp.where(lane < key_size // 2, -1.0, 1.0)[None, :]
    decay = jnp.exp(jnp.log1p(-jnp.exp2(-5.0 - 7.0 * tp_index.astype(F32) / (tp_count - 1))))
    keep, give, new_state = call(
        retention_kernel,
        (
            shaped((own_blocks, rows, 128), F32),
            shaped((own_blocks, rows, 128), BF),
            shaped((rows, key_size, value_size), F32),
        ),
        (
            tokens,
            norm1_gain.reshape(1, width),
            cosine,
            sine,
            decay.reshape(1),
            query_weight,
            key_weight,
            value_weight,
            state.reshape(rows, key_size, value_size),
            out_weight,
        ),
        10_000_000_000,
        scratch=(
            pltpu.VMEM(query_weight.shape, BF),
            pltpu.VMEM(key_weight.shape, BF),
            pltpu.VMEM(value_weight.shape, BF),
            pltpu.VMEM((rows, key_size, value_size), F32),
            pltpu.VMEM(out_weight.shape, BF),
            pltpu.VMEM((rows, key_size, value_size), F32),
            pltpu.VMEM((blocks, rows, 128), F32),
            pltpu.SemaphoreType.DMA((6,)),
        ),
        specs=[vmem, vmem, vmem, vmem, smem, hbm, hbm, hbm, hbm, hbm],
        out_specs=(vmem, vmem, hbm),
        vmem=FULL,
    )
    route_count = route_ids.shape[1]
    route_flat = route_ids.reshape(-1)
    same = (route_flat[:, None] == route_flat[None, :]).astype(jnp.int32)
    number = jnp.arange(rows * route_count, dtype=jnp.int32)
    slot_index = jnp.sum(same * (number[None, :] < number[:, None]), axis=1)
    place_of = jnp.where(slot_index < 2, route_flat * 3 + slot_index, -1)
    place_of = place_of.reshape(rows, route_count)
    in_row = jnp.arange(3 * ep_count, dtype=jnp.int32)
    row_kind = (in_row // 12) * 3 + in_row % 3
    slot_kind = (jnp.arange(ep_count, dtype=jnp.int32) // 4) * 3 + lax.axis_index("c")
    weighted = jnp.sum(
        jnp.where(place_of[:, :, None] == slot_kind, route_weights[:, :, None], 0.0), axis=1
    )
    token = jnp.arange(own_blocks * rows, dtype=jnp.int32) % rows
    tiled = jnp.tile(place_of, (own_blocks, 1))
    chosen = jnp.any(tiled[None] == row_kind[:, None, None], axis=2) | (
        (in_row[:, None] % 3 == 2) & (token[None, :] == x_index)
    )
    select = chosen.astype(F32)[:, None, :]

    sent = call(
        pair_kernel,
        shaped((x_count, own_blocks, rows, 128), BF),
        (keep, swap(give)),
        1_000_000,
    )
    pairs = lax.all_to_all(sent, "x", 0, 0, tiled=True)

    outgoing, own = call(
        dispatch_kernel,
        (shaped((3 * ep_count * own_blocks, 128), BF), shaped((rows, 128), F32)),
        (pairs, tokens, select),
        1_000_000_000,
        scratch=(pltpu.VMEM((own_blocks, rows, 128), F32),),
    )
    arrived = lax.all_to_all(outgoing.reshape(ep_count, 3 * own_blocks, 128), EP, 0, 0, tiled=True)
    mine = arrived.reshape(ep_count, 3, own_blocks, 128).transpose(1, 0, 2, 3)
    mine = mine.reshape(3 * ep_count, width // 2)
    message = shaped((ep_count, 7 * 128), F32)
    kept, given = call(
        first_kernel,
        (message, message),
        (
            mine,
            norm2_gain.reshape(blocks, 128),
            branch_gate.reshape(blocks, 128),
            gate_rows,
            up_rows,
            traded,
            dense_parts,
        ),
        2_000_000_000,
        scratch=(
            pltpu.VMEM((2 * ep_count, 640), F32),
            pltpu.VMEM((2 * down.shape[0], width // 2), BF),
            pltpu.SemaphoreType.DMA,
        ),
        specs=[vmem] * 5 + [hbm, vmem],
    )
    result = call(
        second_kernel,
        shaped((ep_count, 3 * width // 2), BF),
        (kept, swap(given), down, traded, dense_parts),
        2_000_000_000,
        scratch=(
            pltpu.VMEM((2 * down.shape[0], width // 2), BF),
            pltpu.SemaphoreType.DMA,
        ),
        specs=[vmem] * 3 + [hbm, vmem],
    )
    returned = lax.all_to_all(result.reshape(ep_count, 3 * own_blocks, 128), EP, 0, 0, tiled=True)
    total = call(
        combine_kernel,
        shaped((blocks, rows, 128), F32),
        (weighted, returned.reshape(ep_count, 3 * width // 2)),
        100_000_000,
    )
    sums = lax.all_to_all(total, TP, 0, 0, tiled=True)
    layer_out = (own + jnp.sum(sums, axis=0)).astype(BF)
    return (layer_out, new_state.reshape(state.shape))


def solution(mesh):
    split = Mesh(mesh.devices.reshape(8, 8, 8, 2), ("z", "y", "x", "c"))
    return jax.shard_map(
        local,
        mesh=split,
        in_specs=(
            P(EP, None),
            P(EP),
            P(EP, TP, None, None),
            P(),
            P(None, TP),
            P(None, TP),
            P(None, TP),
            P(TP, None),
            P(),
            P(),
            P(EP, None),
            P(EP, None),
            P(EP, None, TP),
            P(EP, None, TP),
            P(EP, TP, None),
            P(TP, EP),
            P(TP, EP),
            P(EP, TP),
        ),
        out_specs=(P(EP, TP), P(EP, TP, None, None)),
        check_vma=False,
    )
```

```python
import jax
import jax.numpy as jnp
from jax import lax
from jax.experimental import pallas as pl
from jax.experimental.pallas import tpu as pltpu
from jax.sharding import Mesh
from jax.sharding import PartitionSpec as P

RMS_EPSILON = 1e-06
GROUP_EPSILON = 1e-05
BF = jnp.bfloat16
F32 = jnp.float32
EP = ("z", "y")
TP = ("x", "c")
NT = (((1,), (1,)), ((), ()))
FULL = 58 << 20
TRADE = 16 << 20


def call(kernel, out_shape, args, flops, scratch=(), specs=None, out_specs=None, vmem=None):
    full = pl.BlockSpec(memory_space=pltpu.VMEM)
    size = sum(a.size * a.dtype.itemsize for a in args)
    return pl.pallas_call(
        kernel,
        out_shape=out_shape,
        in_specs=specs or [full] * len(args),
        out_specs=out_specs or jax.tree.map(lambda _: full, out_shape),
        scratch_shapes=list(scratch),
        compiler_params=pltpu.CompilerParams(vmem_limit_bytes=vmem or 16 << 20),
        cost_estimate=pl.CostEstimate(flops=flops, bytes_accessed=size, transcendentals=0),
    )(*args)


def regroup_kernel(gate_hbm, up_hbm, down_hbm, sent_hbm, packed, sems):
    size = gate_hbm.shape[0]
    count = sent_hbm.shape[0]
    copies = [
        pltpu.make_async_copy(ref, packed.at[pl.ds(size * n, size)], sems.at[count + n])
        for n, ref in enumerate((gate_hbm, up_hbm, down_hbm))
    ]
    for c in copies:
        c.start()
    for c in copies:
        c.wait()
    copies = [pltpu.make_async_copy(packed, sent_hbm.at[n], sems.at[n]) for n in range(count)]
    for c in copies:
        c.start()
    for c in copies:
        c.wait()


def trade_kernel(gate_hbm, up_hbm, down_hbm, out_hbm, sems):
    size, width = down_hbm.shape
    blocks = width // 256
    other = 1 - lax.axis_index("c")
    copies = []
    for n, ref in enumerate((gate_hbm, up_hbm)):
        for k in range(blocks):
            at = pl.ds(pl.multiple_of((2 * k + other) * 128, 128), 128)
            copies.append((ref.at[:, at], (n, pl.ds(128 * k, 128))))
    for n in range(2):
        copies.append((down_hbm.at[:, pl.ds(n * width // 2, width // 2)], (2 + n, slice(None))))
    copies = [
        pltpu.make_async_copy(src, out_hbm.at[pl.ds(size * n, size), lanes], sems.at[i])
        for i, (src, (n, lanes)) in enumerate(copies)
    ]
    for c in copies:
        c.start()
    for c in copies:
        c.wait()


def retention_kernel(
    tokens_ref,
    gain_ref,
    cos_ref,
    sin_ref,
    decay_ref,
    q_hbm,
    k_hbm,
    v_hbm,
    state_hbm,
    out_hbm,
    keep_ref,
    give_ref,
    new_hbm,
    q_w,
    k_w,
    v_w,
    state,
    out_w,
    fresh,
    held,
    sems,
):
    rows, width = tokens_ref.shape
    core = lax.axis_index("c")
    copies = [
        pltpu.make_async_copy(s, d, sems.at[n])
        for n, (s, d) in enumerate(
            ((q_hbm, q_w), (k_hbm, k_w), (v_hbm, v_w), (state_hbm, state), (out_hbm, out_w))
        )
    ]
    for c in copies:
        c.start()
    x = tokens_ref[...].astype(F32)
    inv = lax.rsqrt(jnp.sum(x * x, axis=1, keepdims=True) / width + RMS_EPSILON)
    normed_in = (x * inv * gain_ref[...]).astype(BF)

    def project(n, w):
        copies[n].wait()
        return jnp.dot(normed_in, w[...], preferred_element_type=F32)

    def rotated(v):
        return v * cos_ref[...] + pltpu.roll(v, v.shape[1] // 2, 1) * sin_ref[...]

    query = rotated(project(0, q_w))
    keys = rotated(project(1, k_w)) * q_w.shape[1] ** (-0.5)
    values = project(2, v_w)
    query_t = query.T
    keys_t = keys.T
    copies[3].wait()
    decay = decay_ref[0]
    retained = []
    for i in range(rows):
        new = state[i] * decay + keys_t[:, i : i + 1] * values[i : i + 1, :]
        fresh[i] = new
        retained.append(jnp.sum(query_t[:, i : i + 1] * new, axis=0, keepdims=True))
    back = pltpu.make_async_copy(fresh, new_hbm, sems.at[5])
    back.start()
    retained = jnp.concatenate(retained, axis=0)
    centered = retained - jnp.mean(retained, axis=1, keepdims=True)
    normed = centered * lax.rsqrt(
        jnp.mean(centered * centered, axis=1, keepdims=True) + GROUP_EPSILON
    )
    normed = normed.astype(BF)
    copies[4].wait()
    mix = jnp.dot(normed, out_w[...], preferred_element_type=F32)
    for j in range(width // 128):
        held[j] = mix[:, 128 * j : 128 * j + 128]
    for k in range(width // 256):
        keep_ref[k] = held[2 * k + core]
        give_ref[k] = held[2 * k + 1 - core].astype(BF)
    back.wait()


def pair_kernel(keep_ref, got_ref, sent_ref):
    pair = (keep_ref[...] + got_ref[...].astype(F32)).astype(BF)
    for n in range(sent_ref.shape[0]):
        sent_ref[n] = pair


def dispatch_kernel(
    pairs_ref,
    tokens_ref,
    select_ref,
    gain_ref,
    bias_ref,
    sent_ref,
    own_ref,
    gain_out,
    bias_out,
    held,
):
    rows = tokens_ref.shape[0]
    gain_out[...] = gain_ref[...]
    bias_out[...] = bias_ref[...]
    blocks = pairs_ref.shape[1]
    core = lax.axis_index("c")
    mine = []
    for k in range(blocks):
        at = pl.multiple_of((2 * k + core) * 128, 128)
        m = tokens_ref[:, pl.ds(at, 128)].astype(F32)
        for p in range(pairs_ref.shape[0]):
            m = m + pairs_ref[p, k].astype(F32)
        held[k] = m
        mine.append(m)
    own_ref[...] = held[lax.axis_index("x")]
    mine = jnp.concatenate(mine, axis=0).astype(BF)
    count, _, wide = select_ref.shape
    same = lax.broadcasted_iota(jnp.int32, (blocks, wide), 0) == (
        lax.broadcasted_iota(jnp.int32, (blocks, wide), 1) // rows
    )
    spread = jnp.broadcast_to(select_ref[...], (count, blocks, wide)) * same.astype(F32)[None]
    spread = spread.reshape(count * blocks, wide).astype(BF)
    sent_ref[...] = jnp.dot(spread, mine, preferred_element_type=F32).astype(BF)


def columns(ref, parity, blocks):
    return jnp.concatenate(
        [ref[:, pl.ds(pl.multiple_of((2 * k + parity) * 128, 128), 128)] for k in range(blocks)],
        axis=1,
    )


def gains(ref, k, parity):
    return ref[pl.ds(2 * k + parity, 1), :]


def first_kernel(
    x_ref, gain_ref, bias_ref, gate_ref, up_ref, got_ref, dense_ref, keep_ref, give_ref, sums
):
    count, half_width = x_ref.shape
    third = count // 3
    blocks = half_width // 128
    wide = gate_ref.shape[0]
    size = dense_ref.shape[1] // 3
    core = lax.axis_index("c")
    square = jnp.zeros((count, 128), F32)
    along = jnp.zeros((third, 128), F32)
    parts = []
    for k in range(blocks):
        x = x_ref[:, 128 * k : 128 * k + 128].astype(F32)
        square = square + x * x
        x = x * gains(gain_ref, k, core)
        along = along + x[2 * third :] * gains(bias_ref, k, core)
        parts.append(x.astype(BF))
    x = jnp.concatenate(parts, axis=1)

    def apply(rows, w):
        return lax.dot_general(rows, w, NT, preferred_element_type=F32)

    rows = x[: 2 * third]
    sums[:, :] = jnp.zeros(sums.shape, F32)
    sums[:, 0:wide] = apply(rows, columns(gate_ref, core, blocks))
    sums[:, 128 : 128 + wide] = apply(rows, got_ref[:wide, :])
    sums[:, 256 : 256 + wide] = apply(rows, columns(up_ref, core, blocks))
    sums[:, 384 : 384 + wide] = apply(rows, got_ref[wide : 2 * wide, :])
    sums[:, 512:640] = jnp.broadcast_to(
        jnp.sum(square[: 2 * third], axis=1, keepdims=True), (2 * third, 128)
    )
    own = pl.ds(pl.multiple_of(core * third, third), third)
    other = pl.ds(pl.multiple_of((1 - core) * third, third), third)
    keep_ref[:, :512] = sums[own, :512]
    for p, q in enumerate((1, 0, 3, 2)):
        give_ref[:, 128 * p : 128 * p + 128] = sums[other, 128 * q : 128 * q + 128]
    rows = x[2 * third :]
    lane = lax.broadcasted_iota(jnp.int32, (third, 128), 1)
    both = jnp.where(
        lane < 64,
        jnp.sum(square[2 * third :], axis=1, keepdims=True),
        jnp.sum(along, axis=1, keepdims=True),
    )
    for ref, at in ((keep_ref, own), (give_ref, other)):
        ref[:, 768:896] = jnp.where(lane < 32, sums[at, 512:640], both)
    for n in range(2):
        w = jnp.concatenate(
            [dense_ref[k, size * n : size * n + size, :] for k in range(blocks)], axis=1
        )
        part = jnp.concatenate(
            [apply(rows, w), jnp.zeros((third, 128 - size), F32)], axis=1
        )
        keep_ref[:, 512 + 128 * n : 640 + 128 * n] = part
        give_ref[:, 512 + 128 * n : 640 + 128 * n] = part


def second_kernel(keep_ref, got_ref, down_ref, traded_ref, dense_ref, out_ref):
    wide, width = down_ref.shape
    blocks, size = dense_ref.shape[0], dense_ref.shape[1] // 3
    stats = keep_ref[:, 768:896] + got_ref[:, 768:896]

    def scale(value):
        return lax.rsqrt(value / width + RMS_EPSILON)

    def gated(at, to, count, factor):
        v = (keep_ref[:, at : at + count] + got_ref[:, at : at + count]) * factor
        w = (keep_ref[:, to : to + count] + got_ref[:, to : to + count]) * factor
        return ((v / (1.0 + jnp.exp(-v))) * w).astype(BF)

    factor = scale(stats[:, 0:1])
    own = gated(0, 256, wide, factor)
    other = gated(128, 384, wide, factor)
    for n in range(2):
        at = slice(n * width // 2, (n + 1) * width // 2)
        r = jnp.dot(own, down_ref[:, at], preferred_element_type=F32)
        r = r + jnp.dot(
            other, traded_ref[(2 + n) * wide : (3 + n) * wide, :], preferred_element_type=F32
        )
        out_ref[:, at] = r.astype(BF)
    factor = scale(stats[:, 32:33])
    branch = jax.nn.sigmoid(stats[:, 64:65] * factor)
    hidden = gated(512, 640, size, factor)
    w = jnp.concatenate([dense_ref[k, 2 * size :, :] for k in range(blocks)], axis=1)
    r = branch * jnp.dot(hidden, w, preferred_element_type=F32)
    out_ref[:, width:] = r.astype(BF)


def combine_kernel(weight_ref, back_ref, out_ref):
    rows = weight_ref.shape[0]
    blocks = out_ref.shape[0]
    width = 128 * blocks
    core = lax.axis_index("c")
    weight = weight_ref[...]
    high = weight.astype(BF)
    low = (weight - high.astype(F32)).astype(BF)
    back = back_ref[:, :width]
    total = jnp.dot(high, back, preferred_element_type=F32) + jnp.dot(
        low, back, preferred_element_type=F32
    )
    for j in range(blocks):
        out_ref[j] = total[:, 128 * j : 128 * j + 128]
    here = lax.broadcasted_iota(jnp.int32, (rows, 128), 0) == lax.axis_index("x")
    for k in range(blocks // 2):
        dense = back_ref[:, width + 128 * k : width + 128 * k + 128].astype(F32)
        dense = jnp.sum(dense, axis=0, keepdims=True)
        out_ref[2 * k + core] = out_ref[2 * k + core] + jnp.where(here, dense, 0.0)


def swap(x):
    return lax.ppermute(x, "c", [(0, 1), (1, 0)])


def local(
    tokens,
    past_lengths,
    state,
    norm1_gain,
    query_weight,
    key_weight,
    value_weight,
    out_weight,
    norm2_gain,
    branch_gate,
    route_ids,
    route_weights,
    expert_gate,
    expert_up,
    expert_down,
    dense_gate,
    dense_up,
    dense_down,
):
    rows, width = tokens.shape
    x_count = lax.axis_size("x")
    tp_count = 2 * x_count
    ep_count = lax.axis_size(EP)
    x_index = lax.axis_index("x")
    tp_index = lax.axis_index(TP)
    blocks = width // 128
    own_blocks = blocks // 2
    key_size = query_weight.shape[1]
    value_size = value_weight.shape[1]
    smem = pl.BlockSpec(memory_space=pltpu.SMEM)
    vmem = pl.BlockSpec(memory_space=pltpu.VMEM)
    hbm = pl.BlockSpec(memory_space=pltpu.HBM)
    shaped = jax.ShapeDtypeStruct

    size = dense_down.shape[0]
    sent = call(
        regroup_kernel,
        shaped((x_count, 3 * size, 128), BF),
        (dense_gate.T, dense_up.T, dense_down),
        1_000_000,
        scratch=(
            pltpu.VMEM((3 * size, 128), BF),
            pltpu.SemaphoreType.DMA((x_count + 3,)),
        ),
        specs=[hbm, hbm, hbm],
        out_specs=hbm,
        vmem=FULL,
    )
    dense_parts = lax.all_to_all(sent, "x", 0, 0, tiled=True)

    gate_rows, up_rows, down = expert_gate[0].T, expert_up[0].T, expert_down[0]
    traded = swap(
        call(
            trade_kernel,
            pltpu.HBM((4 * down.shape[0], width // 2), BF),
            (gate_rows, up_rows, down),
            1_000_000,
            scratch=(pltpu.SemaphoreType.DMA((blocks + 2,)),),
            specs=[hbm, hbm, hbm],
            out_specs=hbm,
            vmem=TRADE,
        )
    )

    lane = jnp.arange(key_size, dtype=jnp.int32)
    inverse = 10000.0 ** (-(lane % (key_size // 2)).astype(F32) / (key_size // 2))
    angles = past_lengths.astype(F32)[:, None] * inverse[None, :]
    cosine = jnp.cos(angles)
    sine = jnp.sin(angles) * jnp.where(lane < key_size // 2, -1.0, 1.0)[None, :]
    decay = jnp.exp(jnp.log1p(-jnp.exp2(-5.0 - 7.0 * tp_index.astype(F32) / (tp_count - 1))))
    keep, give, new_state = call(
        retention_kernel,
        (
            shaped((own_blocks, rows, 128), F32),
            shaped((own_blocks, rows, 128), BF),
            shaped((rows, key_size, value_size), F32),
        ),
        (
            tokens,
            norm1_gain.reshape(1, width),
            cosine,
            sine,
            decay.reshape(1),
            query_weight,
            key_weight,
            value_weight,
            state.reshape(rows, key_size, value_size),
            out_weight,
        ),
        10_000_000_000,
        scratch=(
            pltpu.VMEM(query_weight.shape, BF),
            pltpu.VMEM(key_weight.shape, BF),
            pltpu.VMEM(value_weight.shape, BF),
            pltpu.VMEM((rows, key_size, value_size), F32),
            pltpu.VMEM(out_weight.shape, BF),
            pltpu.VMEM((rows, key_size, value_size), F32),
            pltpu.VMEM((blocks, rows, 128), F32),
            pltpu.SemaphoreType.DMA((6,)),
        ),
        specs=[vmem, vmem, vmem, vmem, smem, hbm, hbm, hbm, hbm, hbm],
        out_specs=(vmem, vmem, hbm),
        vmem=FULL,
    )
    route_count = route_ids.shape[1]
    route_flat = route_ids.reshape(-1)
    same = (route_flat[:, None] == route_flat[None, :]).astype(jnp.int32)
    number = jnp.arange(rows * route_count, dtype=jnp.int32)
    slot_index = jnp.sum(same * (number[None, :] < number[:, None]), axis=1)
    place_of = jnp.where(slot_index < 2, route_flat * 3 + slot_index, -1)
    place_of = place_of.reshape(rows, route_count)
    in_row = jnp.arange(3 * ep_count, dtype=jnp.int32)
    row_kind = (in_row // 12) * 3 + in_row % 3
    slot_kind = (jnp.arange(ep_count, dtype=jnp.int32) // 4) * 3 + lax.axis_index("c")
    weighted = jnp.sum(
        jnp.where(place_of[:, :, None] == slot_kind, route_weights[:, :, None], 0.0), axis=1
    )
    token = jnp.arange(own_blocks * rows, dtype=jnp.int32) % rows
    tiled = jnp.tile(place_of, (own_blocks, 1))
    chosen = jnp.any(tiled[None] == row_kind[:, None, None], axis=2) | (
        (in_row[:, None] % 3 == 2) & (token[None, :] == x_index)
    )
    select = chosen.astype(F32)[:, None, :]

    sent = call(
        pair_kernel,
        shaped((x_count, own_blocks, rows, 128), BF),
        (keep, swap(give)),
        1_000_000,
    )
    pairs = lax.all_to_all(sent, "x", 0, 0, tiled=True)

    outgoing, own, gain, bias = call(
        dispatch_kernel,
        (
            shaped((3 * ep_count * own_blocks, 128), BF),
            shaped((rows, 128), F32),
            shaped((blocks, 128), F32),
            shaped((blocks, 128), F32),
        ),
        (pairs, tokens, select, norm2_gain.reshape(blocks, 128), branch_gate.reshape(blocks, 128)),
        1_000_000_000,
        scratch=(pltpu.VMEM((own_blocks, rows, 128), F32),),
    )
    arrived = lax.all_to_all(outgoing.reshape(ep_count, 3 * own_blocks, 128), EP, 0, 0, tiled=True)
    mine = arrived.reshape(ep_count, 3, own_blocks, 128).transpose(1, 0, 2, 3)
    mine = mine.reshape(3 * ep_count, width // 2)
    message = shaped((ep_count, 7 * 128), F32)
    kept, given = call(
        first_kernel,
        (message, message),
        (
            mine,
            gain,
            bias,
            gate_rows,
            up_rows,
            traded,
            dense_parts,
        ),
        2_000_000_000,
        scratch=(pltpu.VMEM((2 * ep_count, 640), F32),),
    )
    result = call(
        second_kernel,
        shaped((ep_count, 3 * width // 2), BF),
        (kept, swap(given), down, traded, dense_parts),
        2_000_000_000,
    )
    returned = lax.all_to_all(result.reshape(ep_count, 3 * own_blocks, 128), EP, 0, 0, tiled=True)
    total = call(
        combine_kernel,
        shaped((blocks, rows, 128), F32),
        (weighted, returned.reshape(ep_count, 3 * width // 2)),
        100_000_000,
    )
    sums = lax.all_to_all(total, TP, 0, 0, tiled=True)
    layer_out = (own + jnp.sum(sums, axis=0)).astype(BF)
    return (layer_out, new_state.reshape(state.shape))


def solution(mesh):
    split = Mesh(mesh.devices.reshape(8, 8, 8, 2), ("z", "y", "x", "c"))
    return jax.shard_map(
        local,
        mesh=split,
        in_specs=(
            P(EP, None),
            P(EP),
            P(EP, TP, None, None),
            P(),
            P(None, TP),
            P(None, TP),
            P(None, TP),
            P(TP, None),
            P(),
            P(),
            P(EP, None),
            P(EP, None),
            P(EP, None, TP),
            P(EP, None, TP),
            P(EP, TP, None),
            P(TP, EP),
            P(TP, EP),
            P(EP, TP),
        ),
        out_specs=(P(EP, TP), P(EP, TP, None, None)),
        check_vma=False,
    )
```
